128 devices in a mesh: sp: 16 (over z, y), dp: 8 (over x, core).
Axes of the slice: x: 4, y: 4, z: 4, core: 2. Of those that a mesh axis runs over, the one named last changes fastest.
Arguments:
- tokens: bfloat16 [8, 4096, 2048], P('dp', 'sp'), may hold values from -6 to 6
- w_query: bfloat16 [2048, 2048], P('dp', 'sp'), may hold values from -0.125 to 0.125
- w_key: bfloat16 [2048, 1024], P('dp', 'sp'), may hold values from -0.125 to 0.125
- w_value: bfloat16 [2048, 1024], P('dp', 'sp'), may hold values from -0.125 to 0.125
- w_out: bfloat16 [2048, 2048], P('dp', 'sp'), may hold values from -0.25 to 0.25
- qk_gain: float32 [2, 128], replicated, may hold values from 0.9 to 24
Outputs:
- mixed_out: bfloat16 [8, 4096, 2048], P('dp', 'sp')
The draws below stay inside these ranges and needn't reach their ends.
All inputs are finite; a program needn't handle non-finite values.
Results may differ from the reference program's by a relative error of at most 0.006.
The reference program's roundings to bfloat16 on the way count: a program that leaves them out, or rounds other values in their place, can miss the bound.
Values may be sent and summed in bfloat16 or wider, within the bound.
A program may use at most 64 MiB of HBM per device.

```python
import math
import jax
import jax.numpy as jnp
from jax import lax

D = 2048
HQ = 16
KV = 8
HD = 128
GRID_W = 64
SEQ = 4096
SEQS = 8


def draw_qk_gain(key, part):
    noise = jnp.clip(jax.random.normal(key, (2, HD), jnp.float32), -3.0, 3.0)
    return 2.0 * (1.0 + 0.18 * noise)


def steps_of(rng, shape, split, low, largest):
    def one(dim, parts):
        heights = jax.random.uniform(jax.random.fold_in(jax.random.fold_in(rng, 6), dim), (parts,), jnp.float32, low / len(split), largest / len(split))
        return jnp.repeat(jnp.exp(heights), shape[dim] // parts).reshape((-1,) + (1,) * (len(shape) - dim - 1))

    level = one(*split[0])
    for cut in split[1:]:
        level = level * one(*cut)
    return level


def normal_values(key, extent, width, limit, cuts=(), held_as=jnp.bfloat16):
    result = jax.random.normal(key, extent, jnp.float32) * width
    if len(cuts) > 0:
        result = steps_of(key, extent, cuts, -0.22, 0.18) * result
    return jnp.clip(result, min=-limit, max=limit).astype(held_as)


def setup_inputs(seed: int = 0) -> dict:
    streams_of = jax.random.split(jax.random.key(seed), 7)
    tokens = normal_values(streams_of[0], (SEQS, SEQ, D), 1.0, 6.0, ((0, 8), (1, 16)))
    w_query = normal_values(streams_of[1], (D, HQ * HD), D ** -0.5, 0.125, ((0, 8), (1, 16)))
    w_key = normal_values(streams_of[2], (D, KV * HD), D ** -0.5, 0.125, ((0, 8), (1, 16)))
    w_value = normal_values(streams_of[3], (D, KV * HD), D ** -0.5, 0.125, ((0, 8), (1, 16)))
    w_out = normal_values(streams_of[4], (HQ * HD, D), (HQ * HD // 4) ** -0.5, 0.25, ((0, 8), (1, 16)))
    qk_gain = draw_qk_gain(jax.random.fold_in(streams_of[6], 71), 0)
    return dict(tokens=tokens, w_query=w_query, w_key=w_key, w_value=w_value, w_out=w_out, qk_gain=qk_gain)


ROPE_BASE = 10000.0
EPS = 1e-06

def angles(positions):
    quarter = jnp.arange(0, HD // 2, 2, dtype=jnp.float32)
    inv_freq = ROPE_BASE ** (-quarter / (HD // 2))
    row_pos = (positions // GRID_W).astype(jnp.float32)
    col_pos = (positions % GRID_W).astype(jnp.float32)
    angle_table = jnp.concatenate([row_pos[:, None] * inv_freq, col_pos[:, None] * inv_freq], axis=1)
    return (jnp.cos(angle_table), jnp.sin(angle_table))

def prepare(raw_proj, gain_row, cosine, sine_table):
    normed = raw_proj * lax.rsqrt(lax.optimization_barrier(jnp.mean(raw_proj * raw_proj, axis=-1, keepdims=True)) + EPS) * gain_row
    pair_view = normed.reshape(raw_proj.shape[:-1] + (HD // 2, 2))
    first_half = pair_view[..., 0]
    second = pair_view[..., 1]
    cos_b = cosine[:, None, :]
    sin_b = sine_table[:, None, :]
    turned = jnp.stack([first_half * cos_b - second * sin_b, first_half * sin_b + second * cos_b], axis=-1)
    return turned.reshape(raw_proj.shape).astype(jnp.bfloat16)

def attend_head(query_rows, key_rows, value_rows):
    seq_len = query_rows.shape[0]
    block_len = math.gcd(seq_len, 512)
    blocks = query_rows.reshape(seq_len // block_len, block_len, HD)

    def one_block(row_block):
        scores = jnp.dot(row_block, key_rows.T, preferred_element_type=jnp.float32) * HD ** (-0.5)
        top_score = lax.optimization_barrier(jnp.max(scores, axis=1, keepdims=True))
        weights = jnp.exp(scores - top_score)
        row_total = lax.optimization_barrier(jnp.sum(weights, axis=1, keepdims=True))
        probs_bf = (weights / row_total).astype(jnp.bfloat16)
        return jnp.dot(probs_bf, value_rows, preferred_element_type=jnp.float32).astype(jnp.bfloat16)
    return lax.map(one_block, blocks).reshape(seq_len, HD)

def reference(tokens, w_query, w_key, w_value, w_out, qk_gain):
    seq_len = tokens.shape[1]
    group_size = HQ // KV
    cosine, sine_table = angles(jnp.arange(seq_len, dtype=jnp.int32))

    def one_sequence(seq_rows):
        query = prepare(jnp.dot(seq_rows, w_query, preferred_element_type=jnp.float32).reshape(seq_len, HQ, HD), qk_gain[0], cosine, sine_table)
        key_all = prepare(jnp.dot(seq_rows, w_key, preferred_element_type=jnp.float32).reshape(seq_len, KV, HD), qk_gain[1], cosine, sine_table)
        value = jnp.dot(seq_rows, w_value, preferred_element_type=jnp.float32).astype(jnp.bfloat16).reshape(seq_len, KV, HD)
        query_heads = jnp.transpose(query, (1, 0, 2))
        key_heads = jnp.repeat(jnp.transpose(key_all, (1, 0, 2)), group_size, axis=0)
        value_heads = jnp.repeat(jnp.transpose(value, (1, 0, 2)), group_size, axis=0)
        attended = lax.map(lambda triple: attend_head(triple[0], triple[1], triple[2]), (query_heads, key_heads, value_heads))
        attended = jnp.transpose(attended, (1, 0, 2)).reshape(seq_len, HQ * HD)
        return jnp.dot(attended, w_out, preferred_element_type=jnp.float32).astype(jnp.bfloat16)
    return lax.map(one_sequence, tokens)
```

```python
import functools
import math

import jax
import jax.numpy as jnp
import numpy as np
from jax import lax
from jax.experimental import pallas as pl
from jax.experimental.pallas import tpu as pltpu
from jax.sharding import PartitionSpec as P

HQ = 16
KV = 8
HD = 128
GRID_W = 64
ROPE_BASE = 10000.0
EPS = 1e-06
ROWS = 256
BF = jnp.bfloat16
F32 = jnp.float32


def rope_tables():
    quarter = np.arange(0, HD // 2, 2, dtype=np.float32)
    inv_freq = np.float32(ROPE_BASE) ** (-quarter / np.float32(HD // 2))
    angle = np.arange(GRID_W, dtype=np.float32)[:, None] * inv_freq.astype(np.float32)
    angle = np.repeat(angle, 2, axis=1).astype(np.float64)
    angle = np.concatenate([angle, angle], axis=1)
    return np.cos(angle).astype(np.float32), np.sin(angle).astype(np.float32)


def kernel(
    tok_hbm, wqkv_hbm, wo_hbm, gain_ref, cos_ref, sin_ref,
    out_ref,
    X, W, WO, QT, KVB, S, ACC, AO, ATT,
    loc, tok_s, tok_r, wy_s, wy_r, wx_s, wx_r, wp_s, wp_r,
    oz_s, oz_r, oy_s, oy_r, ox_s, ox_r, op_s, op_r,
    kv_s, kv_r, at_s, at_r,
):
    sp = lax.axis_index("sp")
    dp = lax.axis_index("dp")
    z, y = sp // 4, sp % 4
    x, c = dp // 2, dp % 2

    def ring(v, d):
        return (v + d + 4) % 4

    def to(src, dst, ss, rs, dz=0, dy=0, dx=0, other=False):
        return pltpu.make_async_remote_copy(
            src_ref=src, dst_ref=dst, send_sem=ss, recv_sem=rs,
            device_id={
                "sp": ring(z, dz) * 4 + ring(y, dy),
                "dp": ring(x, dx) * 2 + ((1 - c) if other else c),
            },
            device_id_type=pl.DeviceIdType.MESH,
        )

    barrier = pltpu.get_barrier_semaphore()
    for kw in (
        dict(dz=1), dict(dz=-1), dict(dz=2), dict(dy=1), dict(dy=-1), dict(dy=2),
        dict(dx=1), dict(dx=-1), dict(other=True),
    ):
        pl.semaphore_signal(
            barrier, inc=1,
            device_id={
                "sp": ring(z, kw.get("dz", 0)) * 4 + ring(y, kw.get("dy", 0)),
                "dp": ring(x, kw.get("dx", 0)) * 2 + ((1 - c) if kw.get("other") else c),
            },
            device_id_type=pl.DeviceIdType.MESH,
        )
    pl.semaphore_wait(barrier, 9)

    lo, hi = pl.ds(0, 128), pl.ds(128, 128)

    def tok(i):
        own = X.at[z]
        if i == 0:
            return to(tok_hbm.at[0, lo], own.at[lo], tok_s.at[0], tok_r.at[0], dz=1)
        if i == 1:
            return to(tok_hbm.at[0, hi], own.at[hi], tok_s.at[1], tok_r.at[1], dz=1)
        if i == 3:
            return to(tok_hbm.at[0, hi], own.at[hi], tok_s.at[3], tok_r.at[3], dz=-1)
        if i == 4:
            return to(tok_hbm.at[0, lo], own.at[lo], tok_s.at[4], tok_r.at[4], dz=-1)
        if i == 2:
            b = X.at[ring(z, -1), lo]
            return to(b, b, tok_s.at[2], tok_r.at[2], dz=1)
        b = X.at[ring(z, 1), hi]
        return to(b, b, tok_s.at[5], tok_r.at[5], dz=-1)

    def tok_in(i):
        src = {0: -1, 1: -1, 2: 2, 3: 1, 4: 1, 5: 2}[i]
        half = {0: lo, 1: hi, 2: lo, 3: hi, 4: lo, 5: hi}[i]
        b = X.at[ring(z, src), half]
        return to(b, b, tok_s.at[i], tok_r.at[i], dz=1)

    DY = (1, -1, 2)

    def wy(i):
        return to(wqkv_hbm, W.at[dp, y], wy_s.at[i], wy_r.at[i], dy=DY[i])

    def wy_in(i):
        b = W.at[dp, ring(y, -DY[i])]
        return to(b, b, wy_s.at[i], wy_r.at[i], dy=1)

    def wblk(r, dx):
        return W.at[ring(x, dx) * 2 + c, ring(y, r)]

    def wx(r, k):
        ss, rs = wx_s.at[r, k], wx_r.at[r, k]
        if k == 0 or k == 1:
            b = wblk(r, 0)
            return to(b, b, ss, rs, dx=1 if k == 0 else -1)
        if k == 2:
            b = wblk(r, -1).at[lo]
            return to(b, b, ss, rs, dx=1)
        b = wblk(r, 1).at[hi]
        return to(b, b, ss, rs, dx=-1)

    def wx_in(r, k):
        ss, rs = wx_s.at[r, k], wx_r.at[r, k]
        b = (wblk(r, -1), wblk(r, 1), wblk(r, 2).at[lo], wblk(r, 2).at[hi])[k]
        return to(b, b, ss, rs, dx=1)

    DXK = (0, -1, 1, 2)

    def wp(r, k):
        b = W.at[ring(x, DXK[k]) * 2 + c, ring(y, r)]
        return to(b, b, wp_s.at[r, k], wp_r.at[r, k], other=True)

    def wp_in(r, k):
        b = W.at[ring(x, DXK[k]) * 2 + (1 - c), ring(y, r)]
        return to(b, b, wp_s.at[r, k], wp_r.at[r, k], other=True)

    def oz(i):
        return to(wo_hbm, WO.at[dp, y, z], oz_s.at[i], oz_r.at[i], dz=DY[i])

    def oz_in(i):
        b = WO.at[dp, y, ring(z, -DY[i])]
        return to(b, b, oz_s.at[i], oz_r.at[i], dz=1)

    def oy(i):
        b = WO.at[dp, y]
        return to(b, b, oy_s.at[i], oy_r.at[i], dy=DY[i])

    def oy_in(i):
        b = WO.at[dp, ring(y, -DY[i])]
        return to(b, b, oy_s.at[i], oy_r.at[i], dy=1)

    y01, y23 = pl.ds(0, 2), pl.ds(2, 2)

    def ox(k):
        ss, rs = ox_s.at[k], ox_r.at[k]
        if k < 2:
            b = WO.at[dp]
            return to(b, b, ss, rs, dx=1 if k == 0 else -1)
        if k == 2:
            b = WO.at[ring(x, -1) * 2 + c, y01]
            return to(b, b, ss, rs, dx=1)
        b = WO.at[ring(x, 1) * 2 + c, y23]
        return to(b, b, ss, rs, dx=-1)

    def ox_in(k):
        far = ring(x, 2) * 2 + c
        b = (
            WO.at[ring(x, -1) * 2 + c], WO.at[ring(x, 1) * 2 + c],
            WO.at[far, y01], WO.at[far, y23],
        )[k]
        return to(b, b, ox_s.at[k], ox_r.at[k], dx=1)

    def op(k):
        b = WO.at[ring(x, DXK[k]) * 2 + c]
        return to(b, b, op_s.at[k], op_r.at[k], other=True)

    def op_in(k):
        b = WO.at[ring(x, DXK[k]) * 2 + (1 - c)]
        return to(b, b, op_s.at[k], op_r.at[k], other=True)

    def kvc(r, k):
        ss, rs = kv_s.at[r, k], kv_r.at[r, k]
        zz = ring(z, r)
        if k < 2:
            b = KVB.at[y * 4 + zz]
            return to(b, b, ss, rs, dy=1 if k == 0 else -1)
        if k == 2:
            b = KVB.at[ring(y, -1) * 4 + zz, 0]
            return to(b, b, ss, rs, dy=1)
        b = KVB.at[ring(y, 1) * 4 + zz, 1]
        return to(b, b, ss, rs, dy=-1)

    def kvc_in(r, k):
        zz = ring(z, r)
        b = (
            KVB.at[ring(y, -1) * 4 + zz], KVB.at[ring(y, 1) * 4 + zz],
            KVB.at[ring(y, 2) * 4 + zz, 0], KVB.at[ring(y, 2) * 4 + zz, 1],
        )[k]
        return to(b, b, kv_s.at[r, k], kv_r.at[r, k], dy=1)

    def at(r, h):
        return to(
            AO.at[r - 1, h], ATT.at[z, h], at_s.at[r - 1, h], at_r.at[r - 1, h], dz=r
        )

    def at_in(r, h):
        b = ATT.at[ring(z, -r), h]
        return to(b, b, at_s.at[r - 1, h], at_r.at[r - 1, h], dz=1)

    copy_x = pltpu.make_async_copy(tok_hbm.at[0], X.at[z], loc.at[0])
    copy_w = pltpu.make_async_copy(wqkv_hbm, W.at[dp, y], loc.at[1])
    copy_o = pltpu.make_async_copy(wo_hbm, WO.at[dp, y, z], loc.at[2])
    copy_w.start()
    for i in range(3):
        wy(i).start()
    tok(0).start()
    tok(3).start()
    copy_o.start()
    for i in range(3):
        oz(i).start()
    tok(1).start()
    tok(4).start()
    copy_x.start()

    copy_w.wait()
    for r in (0, 3, 1, 2):
        if r:
            wy_in({3: 0, 1: 1, 2: 2}[r]).wait_recv()
        wx(r, 0).start()
        wx(r, 1).start()
        wp(r, 0).start()
    copy_o.wait()
    for i in range(3):
        oz_in(i).wait_recv()
    for i in range(3):
        oy(i).start()
    for r in (0, 3, 1, 2):
        wx_in(r, 0).wait_recv()
        wx(r, 2).start()
        wp(r, 1).start()
        wx_in(r, 1).wait_recv()
        wx(r, 3).start()
        wp(r, 2).start()
        if r == 3:
            tok_in(0).wait_recv()
            tok(2).start()
            tok_in(3).wait_recv()
            tok(5).start()
    for i in range(3):
        oy_in(i).wait_recv()
    ox(0).start()
    ox(1).start()
    op(0).start()
    for r in (0, 3, 1, 2):
        wx_in(r, 2).wait_recv()
        wx_in(r, 3).wait_recv()
        wp(r, 3).start()
    for r in (0, 3, 1, 2):
        for k in range(4):
            wp_in(r, k).wait_recv()
    copy_x.wait()

    lane = lax.broadcasted_iota(jnp.int32, (64, HD), 1)
    low64 = lane < 64
    even = lane % 2 == 0

    def normed_turned(raw, gain, cosv, sin_a, sin_b):
        n = raw * lax.rsqrt(jnp.mean(raw * raw, axis=1, keepdims=True) + EPS) * gain
        return n * cosv + (pltpu.roll(n, HD - 1, 1) * sin_a + pltpu.roll(n, 1, 1) * sin_b)

    def project_slot(s, carry):
        r = s ^ (s >> 1)
        zz = lax.rem(z + r, 4)

        @pl.when(s == 1)
        def _():
            tok_in(3).wait_recv() if False else None
            tok_in(4).wait_recv()

        @pl.when(s == 2)
        def _():
            tok_in(1).wait_recv()

        @pl.when(s == 3)
        def _():
            tok_in(2).wait_recv()
            tok_in(5).wait_recv()

        chunk = y * 4 + zz
        first_row = (zz * 4 + y) * 4

        def one_kv_head(j, carry2):
            raws = []
            for b in range(2):
                raw = jnp.zeros((ROWS, ROWS), F32)
                for k in range(8):
                    raw = raw + jnp.dot(
                        X[zz, :, k * 256:(k + 1) * 256], W[k, 2 * j + b],
                        preferred_element_type=F32,
                    )
                raws.append(raw)
            gq = gain_ref[0:1, :]
            gk = gain_ref[1:2, :]
            for g in range(4):
                sl = slice(g * 64, (g + 1) * 64)
                crow = cos_ref[pl.ds(first_row + g, 1), :]
                srow = sin_ref[pl.ds(first_row + g, 1), :]
                cosv = jnp.where(low64, crow, cos_ref[...])
                sinv = jnp.where(low64, srow, sin_ref[...])
                sin_a = jnp.where(even, -sinv, 0.0)
                sin_b = jnp.where(even, 0.0, sinv)
                for b in range(2):
                    qn = normed_turned(raws[b][sl, 0:HD], gq, cosv, sin_a, sin_b)
                    S[b, sl, 0:HD] = qn
                a0 = raws[0][sl, HD:]
                a1 = raws[1][sl, HD:]
                kk = jnp.where(low64, a0, pltpu.roll(a1, 64, 1))
                vv = jnp.where(low64, pltpu.roll(a0, 64, 1), a1)
                kn = normed_turned(kk, gk, cosv, sin_a, sin_b)
                KVB[chunk, j, 0, sl, :] = kn.astype(BF)
                S[2, sl, 0:HD] = vv
            for b in range(2):
                for half in range(2):
                    hs = slice(half * 128, (half + 1) * 128)
                    QT[zz, 2 * j + b, :, hs] = S[b, hs, 0:HD].T.astype(BF)
            for half in range(2):
                hs = slice(half * 128, (half + 1) * 128)
                KVB[chunk, j, 1, hs, :] = S[2, hs, 0:HD].T.astype(BF)
            return carry2

        lax.fori_loop(0, 2, one_kv_head, 0)

        for r_static in range(4):
            @pl.when(r == r_static)
            def _():
                kvc(r_static, 0).start()
                kvc(r_static, 1).start()
        return carry

    lax.fori_loop(0, 4, project_slot, 0)

    for r in (0, 1, 3, 2):
        kvc_in(r, 0).wait_recv()
        kvc(r, 2).start()
        kvc_in(r, 1).wait_recv()
        kvc(r, 3).start()
    for r in (0, 1, 3, 2):
        kvc_in(r, 2).wait_recv()
        kvc_in(r, 3).wait_recv()

    cs = HD ** (-0.5) * math.log2(math.e)
    NEG = jnp.full((8, 256), -jnp.inf, F32)

    def tile_of(i):
        r = lax.rem(i // 4 + 1, 4)
        return r, lax.rem(z + r, 4), lax.rem(i, 4)

    def score_chunk(ck, kvh, qt, m8):
        s_new = jnp.dot(KVB[ck, kvh, 0], qt, preferred_element_type=F32)
        S[ck] = s_new
        return jnp.maximum(m8, jnp.max(s_new.reshape(32, 8, 256), axis=0))

    def first_scores(ck, m8):
        _, zz, h = tile_of(0)
        return score_chunk(ck, h // 2, QT[zz, h], m8)

    m_first = lax.fori_loop(0, 16, first_scores, NEG)

    def tile(i, m8):
        r, zz, h = tile_of(i)
        nxt = lax.rem(i + 1, 16)
        _, zn, hn = tile_of(nxt)
        kvh, kvn = h // 2, hn // 2
        mb = jnp.broadcast_to(jnp.max(m8, axis=0, keepdims=True), (8, 256))
        ACC[...] = jnp.zeros_like(ACC)

        def four(c4, carry):
            m_new, l8 = carry
            pv = None
            for j in range(4):
                ck = c4 * 4 + j
                p = jnp.exp2((S[ck].reshape(32, 8, 256) - mb[None]) * cs)
                l8 = l8 + jnp.sum(p, axis=0)
                vt = jnp.concatenate(
                    [KVB[ck, kvh, 1, 0:128, :], KVB[ck, kvh, 1, 128:256, :]], axis=1
                )
                d = jnp.dot(vt, p.reshape(256, 256).astype(BF), preferred_element_type=F32)
                pv = d if pv is None else pv + d
                m_new = score_chunk(ck, kvn, QT[zn, hn], m_new)
            ACC[...] += pv
            return m_new, l8

        m_new, l8 = lax.fori_loop(0, 4, four, (NEG, jnp.zeros((8, 256), F32)))
        inv = 1.0 / jnp.sum(l8, axis=0, keepdims=True)
        o = (ACC[...] * inv).T.astype(BF)

        @pl.when(r == 0)
        def _():
            ATT[z, h] = o

        for r_static in range(1, 4):
            @pl.when(r == r_static)
            def _():
                AO[r_static - 1, h] = o
                at(r_static, h).start()

        @pl.when(i == 6)
        def _():
            ox_in(0).wait_recv()
            ox(2).start()
            op(1).start()
            ox_in(1).wait_recv()
            ox(3).start()
            op(2).start()

        @pl.when(i == 13)
        def _():
            ox_in(2).wait_recv()
            ox_in(3).wait_recv()
            op(3).start()

        return m_new

    lax.fori_loop(0, 16, tile, m_first)

    for k in range(4):
        op_in(k).wait_recv()
    for r in range(1, 4):
        for h in range(4):
            at_in(r, h).wait_recv()

    def out_block(n, carry):
        zc, yc = n // 2, lax.rem(n, 2) * 2
        total = jnp.zeros((ROWS, 256), F32)
        for k in range(8):
            lhs = jnp.concatenate(
                [ATT[k // 2, 2 * (k % 2)], ATT[k // 2, 2 * (k % 2) + 1]], axis=1
            )
            rhs = jnp.concatenate([WO[k, yc, zc], WO[k, yc + 1, zc]], axis=1)
            total = total + jnp.dot(lhs, rhs, preferred_element_type=F32)
        out_ref[:, pl.ds(pl.multiple_of(n * 256, 256), 256)] = total.astype(BF)
        return carry

    lax.fori_loop(0, 8, out_block, 0)

    for i in range(6):
        tok(i).wait_send()
    for i in range(3):
        wy(i).wait_send()
        oz(i).wait_send()
        oy(i).wait_send()
    for r in range(4):
        for k in range(4):
            wx(r, k).wait_send()
            wp(r, k).wait_send()
            kvc(r, k).wait_send()
    for k in range(4):
        ox(k).wait_send()
        op(k).wait_send()
    for r in range(1, 4):
        for h in range(4):
            at(r, h).wait_send()


def on_device(tokens, w_query, w_key, w_value, w_out, qk_gain):
    wqkv = jnp.concatenate([w_query, w_key, w_value], axis=1)
    cos_t, sin_t = rope_tables()
    any_ = pl.BlockSpec(memory_space=pl.ANY)
    vm = pl.BlockSpec(memory_space=pltpu.VMEM)
    dma = pltpu.SemaphoreType.DMA
    out = pl.pallas_call(
        kernel,
        out_shape=jax.ShapeDtypeStruct((ROWS, 2048), BF),
        in_specs=[any_, any_, any_, vm, vm, vm],
        out_specs=vm,
        scratch_shapes=[
            pltpu.VMEM((4, ROWS, 2048), BF),
            pltpu.VMEM((8, 4, ROWS, 256), BF),
            pltpu.VMEM((8, 4, 4, ROWS, 128), BF),
            pltpu.VMEM((4, 4, HD, ROWS), BF),
            pltpu.VMEM((16, 2, 2, ROWS, HD), BF),
            pltpu.VMEM((16, ROWS, ROWS), F32),
            pltpu.VMEM((HD, ROWS), F32),
            pltpu.VMEM((3, 4, ROWS, HD), BF),
            pltpu.VMEM((4, 4, ROWS, HD), BF),
            dma((3,)),
            dma((6,)), dma((6,)),
            dma((3,)), dma((3,)),
            dma((4, 4)), dma((4, 4)),
            dma((4, 4)), dma((4, 4)),
            dma((3,)), dma((3,)),
            dma((3,)), dma((3,)),
            dma((4,)), dma((4,)),
            dma((4,)), dma((4,)),
            dma((4, 4)), dma((4, 4)),
            dma((3, 4)), dma((3, 4)),
        ],
        compiler_params=pltpu.CompilerParams(
            collective_id=0, has_side_effects=True, vmem_limit_bytes=56 * 1024 * 1024
        ),
    )(tokens, wqkv, w_out, qk_gain, jnp.asarray(cos_t), jnp.asarray(sin_t))
    return out[None]


def solution(mesh):
    in_specs = (
        P("dp", "sp", None),
        P("dp", "sp"),
        P("dp", "sp"),
        P("dp", "sp"),
        P("dp", "sp"),
        P(),
    )
    out_specs = P("dp", "sp", None)
    return jax.shard_map(
        on_device, mesh=mesh, in_specs=in_specs, out_specs=out_specs, check_vma=False
    )
```

```python
import functools
import math

import jax
import jax.numpy as jnp
import numpy as np
from jax import lax
from jax.experimental import pallas as pl
from jax.experimental.pallas import tpu as pltpu
from jax.sharding import PartitionSpec as P

HQ = 16
KV = 8
HD = 128
GRID_W = 64
ROPE_BASE = 10000.0
EPS = 1e-06
ROWS = 256
BF = jnp.bfloat16
F32 = jnp.float32


def rope_tables():
    quarter = np.arange(0, HD // 2, 2, dtype=np.float32)
    inv_freq = np.float32(ROPE_BASE) ** (-quarter / np.float32(HD // 2))
    angle = np.arange(GRID_W, dtype=np.float32)[:, None] * inv_freq.astype(np.float32)
    angle = np.repeat(angle, 2, axis=1).astype(np.float64)
    angle = np.concatenate([angle, angle], axis=1)
    return np.cos(angle).astype(np.float32), np.sin(angle).astype(np.float32)


class Ring:
    def __init__(self, copy, slot, half, step, send, recv):
        self.copy, self.slot, self.half, self.step = copy, slot, half, step
        self.send, self.recv = send, recv

    def out(self, k):
        if k == 0 or k == 1:
            block = self.slot(0)
        elif k == 2:
            block = self.half(self.slot(3), 0)
        else:
            block = self.half(self.slot(1), 1)
        return self.copy(block, block, self.send(k), self.recv(k), **self.step(1 if k % 2 == 0 else 3))

    def into(self, k):
        far = self.slot(2)
        block = (self.slot(3), self.slot(1), self.half(far, 0), self.half(far, 1))[k]
        return self.copy(block, block, self.send(k), self.recv(k), **self.step(1))


def kernel(
    tok_hbm, wq_hbm, wk_hbm, wv_hbm, wo_hbm, gain_ref, cos_ref, sin_ref,
    out_ref,
    X, W, WO, QT, KVB, S, ACC, MX, LS, AO, ATT,
    loc, tok_s, tok_r, w1_s, w1_r, w2_s, w2_r, wp_s, wp_r,
    oz_s, oz_r, oy_s, oy_r, ox_s, ox_r, op_s, op_r,
    kv_s, kv_r, at_s, at_r,
):
    sp = lax.axis_index("sp")
    dp = lax.axis_index("dp")
    z, y = sp // 4, sp % 4
    x, c = dp // 2, dp % 2

    def ring(v, d):
        return (v + d + 4) % 4

    def device(dz=0, dy=0, dx=0, other=False):
        return {
            "sp": ring(z, dz) * 4 + ring(y, dy),
            "dp": ring(x, dx) * 2 + ((1 - c) if other else c),
        }

    def to(src, dst, ss, rs, **where):
        return pltpu.make_async_remote_copy(
            src_ref=src, dst_ref=dst, send_sem=ss, recv_sem=rs,
            device_id=device(**where), device_id_type=pl.DeviceIdType.MESH,
        )

    lo, hi = pl.ds(0, 128), pl.ds(128, 128)

    local = [
        (wq_hbm, W.at[dp, y, 0]),
        (wk_hbm.at[:, lo], W.at[dp, y, 1, pl.ds(0, 64)]),
        (wk_hbm.at[:, hi], W.at[dp, y, 1, pl.ds(128, 64)]),
        (wv_hbm.at[:, lo], W.at[dp, y, 1, pl.ds(64, 64)]),
        (wv_hbm.at[:, hi], W.at[dp, y, 1, pl.ds(192, 64)]),
        (wo_hbm, WO.at[dp, y, z]),
        (tok_hbm.at[0], X.at[0]),
    ]
    local = [pltpu.make_async_copy(a, b, loc.at[i]) for i, (a, b) in enumerate(local)]
    for one in local:
        one.start()

    barrier = pltpu.get_barrier_semaphore()
    for where in (
        dict(dz=1), dict(dz=3), dict(dz=2), dict(dy=1), dict(dy=3), dict(dx=1), dict(dx=3),
        dict(other=True),
    ):
        pl.semaphore_signal(
            barrier, inc=1, device_id=device(**where), device_id_type=pl.DeviceIdType.MESH
        )
    pl.semaphore_wait(barrier, 8)

    def tok(i):
        dst = (X.at[1, lo], X.at[1, hi], X.at[2, hi], X.at[2, lo], X.at[3, lo], X.at[3, hi])[i]
        src = (
            tok_hbm.at[0, lo], tok_hbm.at[0, hi], tok_hbm.at[0, hi], tok_hbm.at[0, lo],
            X.at[1, lo], X.at[1, hi],
        )[i]
        return to(src, dst, tok_s.at[i], tok_r.at[i], dz=1 if i % 2 == 0 else 3)

    def set_off(v, half):
        gray = v ^ (v >> 1)
        return gray if half else (4 - gray) % 4

    def wslot(cc, d1, d2):
        return W.at[ring(x, d2 * (1 - cc) + d1 * cc) * 2 + cc, ring(y, d1 * (1 - cc) + d2 * cc)]

    first_half = lambda ref, i: ref.at[i]
    w1 = Ring(
        to, lambda d: wslot(c, d, 0), first_half, lambda d: dict(dy=d * (1 - c), dx=d * c),
        lambda k: w1_s.at[k], lambda k: w1_r.at[k],
    )
    w2 = [
        Ring(
            to, lambda d, r=r: wslot(c, r, d), first_half,
            lambda d: dict(dy=d * c, dx=d * (1 - c)),
            lambda k, r=r: w2_s.at[r, k], lambda k, r=r: w2_r.at[r, k],
        )
        for r in range(4)
    ]

    def wp(r, d):
        b = wslot(c, r, d)
        return to(b, b, wp_s.at[r, d], wp_r.at[r, d], other=True)

    def wp_in(r, d):
        b = wslot(1 - c, r, d)
        return to(b, b, wp_s.at[r, d], wp_r.at[r, d], other=True)

    def oz(d):
        return to(wo_hbm, WO.at[dp, y, z], oz_s.at[d - 1], oz_r.at[d - 1], dz=d)

    def oz_in(d):
        b = WO.at[dp, y, ring(z, -d)]
        return to(b, b, oz_s.at[d - 1], oz_r.at[d - 1], dz=1)

    two = lambda ref, i: ref.at[pl.ds(2 * i, 2)]
    oy = Ring(
        to, lambda d: WO.at[dp, ring(y, d)], two,
        lambda d: dict(dy=d), lambda k: oy_s.at[k], lambda k: oy_r.at[k],
    )
    ox = Ring(
        to, lambda d: WO.at[ring(x, d) * 2 + c], two,
        lambda d: dict(dx=d), lambda k: ox_s.at[k], lambda k: ox_r.at[k],
    )

    def op(d):
        b = WO.at[ring(x, d) * 2 + c]
        return to(b, b, op_s.at[d], op_r.at[d], other=True)

    def op_in(d):
        b = WO.at[ring(x, d) * 2 + (1 - c)]
        return to(b, b, op_s.at[d], op_r.at[d], other=True)

    def kvr(v):
        return Ring(
            to, lambda d: KVB.at[ring(y, d) * 4 + v], first_half, lambda d: dict(dy=d),
            lambda k: kv_s.at[v, k], lambda k: kv_r.at[v, k],
        )

    def at(v, h, half):
        rows = hi if half else lo
        return to(
            AO.at[v - 1, h, rows], ATT.at[z, h, rows],
            at_s.at[v - 1, h, half], at_r.at[v - 1, h, half], dz=set_off(v, half),
        )

    def at_in(v, h, half):
        b = ATT.at[ring(z, -set_off(v, half)), h, hi if half else lo]
        return to(b, b, at_s.at[v - 1, h, half], at_r.at[v - 1, h, half], dz=1)

    for d in (2, 1, 3):
        oz(d).start()
    for i in range(4):
        tok(i).start()
    for i in range(5):
        local[i].wait()
    w1.out(0).start()
    w1.out(1).start()
    w2[0].out(0).start()
    w2[0].out(1).start()
    wp(0, 0).start()
    ACC[...] = jnp.zeros_like(ACC)
    LS[...] = jnp.zeros_like(LS)
    MX[...] = jnp.full(MX.shape, -jnp.inf, F32)
    for r, k in ((3, 0), (1, 1)):
        w1.into(k).wait_recv()
        w1.out(k + 2).start()
        w2[r].out(0).start()
        w2[r].out(1).start()
        wp(r, 0).start()
    w1.into(2).wait_recv()
    w1.into(3).wait_recv()
    w2[2].out(0).start()
    w2[2].out(1).start()
    wp(2, 0).start()
    local[5].wait()
    for d in (1, 3, 2):
        oz_in(d).wait_recv()
    oy.out(0).start()
    oy.out(1).start()
    for r in (0, 3, 1, 2):
        for k in range(2):
            w2[r].into(k).wait_recv()
            w2[r].out(k + 2).start()
            wp(r, 3 if k == 0 else 1).start()
    for r in (0, 3, 1, 2):
        w2[r].into(2).wait_recv()
        w2[r].into(3).wait_recv()
        wp(r, 2).start()
    for i in range(2):
        tok(i).wait_recv()
        tok(i + 4).start()
    for k in range(2):
        oy.into(k).wait_recv()
        oy.out(k + 2).start()
    for r in (0, 3, 1, 2):
        for d in (0, 3, 1, 2):
            wp_in(r, d).wait_recv()
    local[6].wait()

    lane = lax.broadcasted_iota(jnp.int32, (64, HD), 1)
    low64 = lane < 64
    even = lane % 2 == 0

    def normed_turned(raw, gain, cosv, sin_a, sin_b):
        n = raw * lax.rsqrt(jnp.mean(raw * raw, axis=1, keepdims=True) + EPS) * gain
        return n * cosv + (pltpu.roll(n, HD - 1, 1) * sin_a + pltpu.roll(n, 1, 1) * sin_b)

    def project(v):
        chunk = y * 4 + v
        gq = gain_ref[0:1, :]
        gk = gain_ref[1:2, :]
        turns = []
        for g in range(4):
            row = (ring(z, set_off(v, g // 2)) * 4 + y) * 4 + g
            cosv = jnp.where(low64, cos_ref[pl.ds(row, 1), :], cos_ref[...])
            sinv = jnp.where(low64, sin_ref[pl.ds(row, 1), :], sin_ref[...])
            turns.append((cosv, jnp.where(even, -sinv, 0.0), jnp.where(even, 0.0, sinv)))
        for j in range(2):
            rawq = jnp.zeros((ROWS, ROWS), F32)
            rawkv = jnp.zeros((ROWS, ROWS), F32)
            for k in range(8):
                rows = X[v, :, k * 256:(k + 1) * 256]
                rq = jnp.concatenate([W[k, 2 * j, 0], W[k, 2 * j + 1, 0]], axis=1)
                rkv = jnp.concatenate(
                    [
                        jnp.concatenate([W[k, b, 1, 0:128], W[k, b, 1, 128:256]], axis=1)
                        for b in (2 * j, 2 * j + 1)
                    ],
                    axis=0,
                )
                rawq = rawq + jnp.dot(rows, rq, preferred_element_type=F32)
                rawkv = rawkv + lax.dot_general(
                    rows, rkv, (((1,), (1,)), ((), ())), preferred_element_type=F32
                )
            for g in range(4):
                sl = slice(g * 64, (g + 1) * 64)
                for b in range(2):
                    S[3 * j + b, sl, 0:HD] = normed_turned(
                        rawq[sl, b * HD:(b + 1) * HD], gq, *turns[g]
                    )
                a0 = rawkv[sl, 0:HD]
                a1 = rawkv[sl, HD:]
                kk = jnp.where(low64, a0, pltpu.roll(a1, 64, 1))
                KVB[chunk, j, 0, sl, :] = normed_turned(kk, gk, *turns[g]).astype(BF)
                S[3 * j + 2, sl, 0:HD] = jnp.where(low64, pltpu.roll(a0, 64, 1), a1)
            for half in range(2):
                hs = slice(half * 128, (half + 1) * 128)
                for b in range(2):
                    QT[v, 2 * j + b, :, hs] = S[3 * j + b, hs, 0:HD].T.astype(BF)
                KVB[chunk, j, 1, hs, :] = S[3 * j + 2, hs, 0:HD].T.astype(BF)

    def project_and_send(v, carry):
        project(v)
        ringv = kvr(v)
        ringv.out(0).start()
        ringv.out(1).start()
        return carry

    def kv_pass_on(v):
        ringv = kvr(v)
        for k in range(2):
            ringv.into(k).wait_recv()
            ringv.out(k + 2).start()

    def kv_far(v):
        ringv = kvr(v)
        ringv.into(2).wait_recv()
        ringv.into(3).wait_recv()

    cs = HD ** (-0.5) * math.log2(math.e)
    NEG = jnp.full((8, 256), -jnp.inf, F32)

    def run_units(n, unit_of, chunks, finish=None, events=()):
        refs = [ring(y, dy) * 4 + v for dy, v in chunks]

        def scores(u, j, m8):
            v, h = unit_of(u)
            s = jnp.dot(KVB[refs[j], h // 2, 0], QT[v, h], preferred_element_type=F32)
            S[j] = s
            return jnp.maximum(m8, jnp.max(s.reshape(32, 8, 256), axis=0))

        m8 = NEG
        for j in range(len(refs)):
            m8 = scores(0, j, m8)

        def unit(u, m8):
            v, h = unit_of(u)
            nxt = jnp.minimum(u + 1, n - 1)
            t = v * 4 + h
            m_old = MX[t]
            m = jnp.maximum(m_old, jnp.broadcast_to(jnp.max(m8, axis=0, keepdims=True), (8, 256)))
            alpha = jnp.exp2((m_old - m) * cs)
            l8 = LS[t] * alpha
            pv = None
            m_next = NEG
            for j in range(len(refs)):
                p = jnp.exp2((S[j].reshape(32, 8, 256) - m[None]) * cs)
                l8 = l8 + jnp.sum(p, axis=0)
                vt = jnp.concatenate(
                    [KVB[refs[j], h // 2, 1, 0:128, :], KVB[refs[j], h // 2, 1, 128:256, :]],
                    axis=1,
                )
                d = jnp.dot(vt, p.reshape(256, 256).astype(BF), preferred_element_type=F32)
                pv = d if pv is None else pv + d
                m_next = scores(nxt, j, m_next)
            acc = (ACC[t].reshape(16, 8, 256) * alpha[None]).reshape(HD, ROWS) + pv
            if finish is None:
                MX[t] = m
                LS[t] = l8
                ACC[t] = acc
            else:
                finish(v, h, acc * (1.0 / jnp.sum(l8, axis=0, keepdims=True)))
            for when, event in events:
                pl.when(u == when)(event)
            return m_next

        lax.fori_loop(0, n, unit, m8)

    def finish(v, h, o):
        rows = o.T.astype(BF)

        @pl.when(v == 0)
        def _():
            ATT[z, h] = rows

        @pl.when(v != 0)
        def _():
            AO[v - 1, h] = rows
            at(v, h, 0).start()
            at(v, h, 1).start()

    def ox_start():
        oy.into(2).wait_recv()
        oy.into(3).wait_recv()
        ox.out(0).start()
        ox.out(1).start()
        op(0).start()

    def ox_pass_on():
        for k in range(2):
            ox.into(k).wait_recv()
            ox.out(k + 2).start()
            op(3 if k == 0 else 1).start()

    def ox_far():
        ox.into(2).wait_recv()
        ox.into(3).wait_recv()
        op(2).start()

    lax.fori_loop(0, 2, project_and_send, 0)
    ox_start()
    tok(2).wait_recv()
    tok(3).wait_recv()
    project_and_send(2, 0)
    kv_pass_on(0)
    own3 = ((0, 0), (0, 1), (0, 2))
    near2 = ((1, 0), (3, 0), (1, 1), (3, 1))
    run_units(12, lambda u: (u // 4, u % 4), own3)
    kv_pass_on(1)
    run_units(12, lambda u: (u // 4, u % 4), near2)
    tok(4).wait_recv()
    tok(5).wait_recv()
    project_and_send(3, 0)
    kv_pass_on(2)
    run_units(4, lambda u: (3, u), own3 + near2)
    kv_far(0)
    kv_far(1)
    run_units(
        16, lambda u: (u // 4, u % 4), ((0, 3), (2, 0), (2, 1), (1, 2), (3, 2)),
        events=((10, lambda: kv_pass_on(3)), (12, ox_pass_on)),
    )
    kv_far(2)
    kv_far(3)
    run_units(
        16, lambda u: (3 - u // 4, u % 4), ((2, 2), (1, 3), (3, 3), (2, 3)),
        finish=finish, events=((14, ox_far),),
    )
    for v in range(1, 4):
        for h in range(4):
            for half in range(2):
                at_in(v, h, half).wait_recv()
    for d in (0, 3, 1, 2):
        op_in(d).wait_recv()

    def out_block(n, carry):
        zc, yc = n // 2, lax.rem(n, 2) * 2
        total = jnp.zeros((ROWS, 256), F32)
        for k in range(8):
            lhs = jnp.concatenate(
                [ATT[k // 2, 2 * (k % 2)], ATT[k // 2, 2 * (k % 2) + 1]], axis=1
            )
            rhs = jnp.concatenate([WO[k, yc, zc], WO[k, yc + 1, zc]], axis=1)
            total = total + jnp.dot(lhs, rhs, preferred_element_type=F32)
        out_ref[:, pl.ds(pl.multiple_of(n * 256, 256), 256)] = total.astype(BF)
        return carry

    lax.fori_loop(0, 8, out_block, 0)
    for i in range(6):
        tok(i).wait_send()
    for d in (1, 2, 3):
        oz(d).wait_send()
    for k in range(4):
        for stage in (w1, oy, ox, *w2, *[kvr(v) for v in range(4)]):
            stage.out(k).wait_send()
        op(k).wait_send()
        for r in range(4):
            wp(r, k).wait_send()
    for v in range(1, 4):
        for h in range(4):
            for half in range(2):
                at(v, h, half).wait_send()


def on_device(tokens, w_query, w_key, w_value, w_out, qk_gain):
    cos_t, sin_t = rope_tables()
    any_ = pl.BlockSpec(memory_space=pl.ANY)
    vm = pl.BlockSpec(memory_space=pltpu.VMEM)
    dma = pltpu.SemaphoreType.DMA
    pair = lambda *shape: [dma(shape), dma(shape)]
    out = pl.pallas_call(
        kernel,
        out_shape=jax.ShapeDtypeStruct((ROWS, 2048), BF),
        in_specs=[any_, any_, any_, any_, any_, vm, vm, vm],
        out_specs=vm,
        scratch_shapes=[
            pltpu.VMEM((4, ROWS, 2048), BF),
            pltpu.VMEM((8, 4, 2, ROWS, HD), BF),
            pltpu.VMEM((8, 4, 4, ROWS, HD), BF),
            pltpu.VMEM((4, 4, HD, ROWS), BF),
            pltpu.VMEM((16, 2, 2, ROWS, HD), BF),
            pltpu.VMEM((7, ROWS, ROWS), F32),
            pltpu.VMEM((16, HD, ROWS), F32),
            pltpu.VMEM((16, 8, ROWS), F32),
            pltpu.VMEM((16, 8, ROWS), F32),
            pltpu.VMEM((3, 4, ROWS, HD), BF),
            pltpu.VMEM((4, 4, ROWS, HD), BF),
            dma((7,)),
            *pair(6), *pair(4), *pair(4, 4), *pair(4, 4),
            *pair(3), *pair(4), *pair(4), *pair(4),
            *pair(4, 4), *pair(3, 4, 2),
        ],
        compiler_params=pltpu.CompilerParams(
            collective_id=0, has_side_effects=True, vmem_limit_bytes=56 * 1024 * 1024
        ),
    )(tokens, w_query, w_key.T, w_value.T, w_out, qk_gain, jnp.asarray(cos_t), jnp.asarray(sin_t))
    return out[None]


def solution(mesh):
    in_specs = (
        P("dp", "sp", None),
        P("dp", "sp"),
        P("dp", "sp"),
        P("dp", "sp"),
        P("dp", "sp"),
        P(),
    )
    out_specs = P("dp", "sp", None)
    return jax.shard_map(
        on_device, mesh=mesh, in_specs=in_specs, out_specs=out_specs, check_vma=False
    )
```

```python
import functools
import math

import jax
import jax.numpy as jnp
import numpy as np
from jax import lax
from jax.experimental import pallas as pl
from jax.experimental.pallas import tpu as pltpu
from jax.sharding import PartitionSpec as P

HQ = 16
KV = 8
HD = 128
GRID_W = 64
ROPE_BASE = 10000.0
EPS = 1e-06
ROWS = 256
BF = jnp.bfloat16
F32 = jnp.float32


def rope_tables():
    quarter = np.arange(0, HD // 2, 2, dtype=np.float32)
    inv_freq = np.float32(ROPE_BASE) ** (-quarter / np.float32(HD // 2))
    angle = np.arange(GRID_W, dtype=np.float32)[:, None] * inv_freq.astype(np.float32)
    angle = np.repeat(angle, 2, axis=1).astype(np.float64)
    angle = np.concatenate([angle, angle], axis=1)
    return np.cos(angle).astype(np.float32), np.sin(angle).astype(np.float32)


class Ring:
    def __init__(self, copy, slot, half, step, send, recv):
        self.copy, self.slot, self.half, self.step = copy, slot, half, step
        self.send, self.recv = send, recv

    def out(self, k):
        if k == 0 or k == 1:
            block = self.slot(0)
        elif k == 2:
            block = self.half(self.slot(3), 0)
        else:
            block = self.half(self.slot(1), 1)
        return self.copy(block, block, self.send(k), self.recv(k), **self.step(1 if k % 2 == 0 else 3))

    def into(self, k):
        far = self.slot(2)
        block = (self.slot(3), self.slot(1), self.half(far, 0), self.half(far, 1))[k]
        return self.copy(block, block, self.send(k), self.recv(k), **self.step(1))


def kernel(
    tok_hbm, wq_hbm, wk_hbm, wv_hbm, wo_hbm, gain_ref, cos_ref, sin_ref,
    out_ref,
    X, W, WO, QT, KVB, S, ACC, MX, LS, AO, ATT, RB, OF, OB,
    loc, tok_s, tok_r, w1_s, w1_r, w2_s, w2_r, wp_s, wp_r,
    o1_s, o1_r, o2_s, o2_r, o3_s, o3_r, op_s, op_r,
    kv_s, kv_r, at_s, at_r, rl_s, rl_r, out_s,
):
    sp = lax.axis_index("sp")
    dp = lax.axis_index("dp")
    z, y = sp // 4, sp % 4
    x, c = dp // 2, dp % 2

    def ring(v, d):
        return (v + d + 4) % 4

    def device(dz=0, dy=0, dx=0, other=False):
        return {
            "sp": ring(z, dz) * 4 + ring(y, dy),
            "dp": ring(x, dx) * 2 + ((1 - c) if other else c),
        }

    def to(src, dst, ss, rs, **where):
        return pltpu.make_async_remote_copy(
            src_ref=src, dst_ref=dst, send_sem=ss, recv_sem=rs,
            device_id=device(**where), device_id_type=pl.DeviceIdType.MESH,
        )

    lo, hi = pl.ds(0, 128), pl.ds(128, 128)

    local = [
        (wq_hbm, W.at[dp, y, 0]),
        (wk_hbm.at[:, lo], W.at[dp, y, 1, pl.ds(0, 64)]),
        (wk_hbm.at[:, hi], W.at[dp, y, 1, pl.ds(128, 64)]),
        (wv_hbm.at[:, lo], W.at[dp, y, 1, pl.ds(64, 64)]),
        (wv_hbm.at[:, hi], W.at[dp, y, 1, pl.ds(192, 64)]),
        (wo_hbm, WO.at[c, x, y, z]),
        (tok_hbm.at[0], X.at[0]),
    ]
    local = [pltpu.make_async_copy(a, b, loc.at[i]) for i, (a, b) in enumerate(local)]
    for one in local:
        one.start()

    barrier = pltpu.get_barrier_semaphore()
    for where in (
        dict(dz=1), dict(dz=3), dict(dz=2), dict(dy=1), dict(dy=3), dict(dy=2), dict(dx=1),
        dict(dx=3), dict(dx=2), dict(other=True),
    ):
        pl.semaphore_signal(
            barrier, inc=1, device_id=device(**where), device_id_type=pl.DeviceIdType.MESH
        )
    pl.semaphore_wait(barrier, 10)

    def tok(i):
        dst = (X.at[1, lo], X.at[1, hi], X.at[2, hi], X.at[2, lo], X.at[3, lo], X.at[3, hi])[i]
        src = (
            tok_hbm.at[0, lo], tok_hbm.at[0, hi], tok_hbm.at[0, hi], tok_hbm.at[0, lo],
            X.at[1, lo], X.at[1, hi],
        )[i]
        return to(src, dst, tok_s.at[i], tok_r.at[i], dz=1 if i % 2 == 0 else 3)

    def set_off(v, half):
        gray = v ^ (v >> 1)
        return gray if half else (4 - gray) % 4

    def wslot(cc, d1, d2, part):
        cc1 = cc * part
        return W.at[
            ring(x, d2 * (1 - cc1) + d1 * cc1) * 2 + cc, ring(y, d1 * (1 - cc1) + d2 * cc1), part
        ]

    first_half = lambda ref, i: ref.at[i]
    row_half = lambda ref, i: ref.at[hi if i else lo]
    w1 = [
        Ring(
            to, lambda d, p=p: wslot(c, d, 0, p), row_half,
            lambda d, p=p: dict(dy=d * (1 - c * p), dx=d * c * p),
            lambda k, p=p: w1_s.at[p, k], lambda k, p=p: w1_r.at[p, k],
        )
        for p in range(2)
    ]
    w2 = [
        [
            Ring(
                to, lambda d, r=r, p=p: wslot(c, r, d, p), row_half,
                lambda d, p=p: dict(dy=d * c * p, dx=d * (1 - c * p)),
                lambda k, r=r, p=p: w2_s.at[p, r, k], lambda k, r=r, p=p: w2_r.at[p, r, k],
            )
            for r in range(4)
        ]
        for p in range(2)
    ]

    def wp(p, r, d):
        b = wslot(c, r, d, p)
        return to(b, b, wp_s.at[p, r, d], wp_r.at[p, r, d], other=True)

    def wp_in(p, r, d):
        b = wslot(1 - c, r, d, p)
        return to(b, b, wp_s.at[p, r, d], wp_r.at[p, r, d], other=True)

    oa, ob, oc = x, y, z

    def o1(d):
        return to(
            wo_hbm, WO.at[c, oa, ob, oc], o1_s.at[d - 1], o1_r.at[d - 1], dz=d
        )

    def o1_in(d):
        b = WO.at[c, oa, ob, ring(oc, -d)]
        return to(b, b, o1_s.at[d - 1], o1_r.at[d - 1], dz=1)

    two = lambda ref, i: ref.at[pl.ds(2 * i, 2)]
    o2 = Ring(
        to, lambda d: WO.at[c, oa, ring(ob, d)], two,
        lambda d: dict(dy=d), lambda k: o2_s.at[k], lambda k: o2_r.at[k],
    )
    o3 = [
        Ring(
            to, lambda d, r=r: WO.at[c, ring(oa, d), ring(ob, r)], two,
            lambda d: dict(dx=d), lambda k, r=r: o3_s.at[r, k], lambda k, r=r: o3_r.at[r, k],
        )
        for r in range(4)
    ]

    def op(r, d):
        b = WO.at[c, ring(oa, d), ring(ob, r)]
        return to(b, b, op_s.at[r, d], op_r.at[r, d], other=True)

    def op_in(r, d):
        b = WO.at[1 - c, ring(oa, d), ring(y, r)]
        return to(b, b, op_s.at[r, d], op_r.at[r, d], other=True)

    def kvc(v, i, landing=False):
        half = (0, 1, 1, 0, 0, 1)[i]
        from_y = ((3, 3, 1, 1, 2, 2) if landing else (0, 0, 0, 0, 3, 1))[i]
        b = KVB.at[ring(y, from_y) * 4 + v, half]
        return to(b, b, kv_s.at[v, i], kv_r.at[v, i], dy=(1, 1, 3, 3, 1, 3)[i])

    def at(v, g, half):
        rows, heads = hi if half else lo, pl.ds(2 * g, 2)
        return to(
            AO.at[v, heads, rows], ATT.at[z, heads, rows],
            at_s.at[v - 1, g, half], at_r.at[v - 1, g, half], dz=set_off(v, half),
        )

    def at_in(v, g, half):
        b = ATT.at[ring(z, -set_off(v, half)), pl.ds(2 * g, 2), hi if half else lo]
        return to(b, b, at_s.at[v - 1, g, half], at_r.at[v - 1, g, half], dz=1)

    def relay_in(g, half):
        heads = pl.ds(2 * g, 2)
        return to(
            AO.at[3, heads, hi if half else lo], RB.at[half, heads],
            rl_s.at[g, half], rl_r.at[g, half], dz=3 if half else 1,
        )

    def relay_out(g, half):
        heads = pl.ds(2 * g, 2)
        return to(
            RB.at[half, heads], ATT.at[ring(z, 1 if half else 3), heads, hi if half else lo],
            at_s.at[2, g, half], at_r.at[2, g, half], dz=3 if half else 1,
        )

    def w1_near(p):
        for k in range(2):
            w1[p].into(k).wait_recv()
            if p == 0:
                w1[p].out(k + 2).start()

    def w1_far(p):
        if p == 0:
            w1[p].into(2).wait_recv()
            w1[p].into(3).wait_recv()
        else:
            w1_across(True).wait_recv()

    def w1_across(landing=False):
        b = wslot(c, 2 if landing else 0, 0, 1)
        return to(b, b, w1_s.at[1, 2], w1_r.at[1, 2], dy=2 * (1 - c), dx=2 * c)

    def w2_send(p, r):
        w2[p][r].out(0).start()
        w2[p][r].out(1).start()
        wp(p, r, 0).start()

    def w2_near(p, r):
        for k in range(2):
            w2[p][r].into(k).wait_recv()
            w2[p][r].out(k + 2).start()
            wp(p, r, 3 if k == 0 else 1).start()

    def w2_far(p, r):
        w2[p][r].into(2).wait_recv()
        w2[p][r].into(3).wait_recv()
        wp(p, r, 2).start()

    def wp_wait(p):
        for r in (0, 3, 1, 2):
            for d in (0, 3, 1, 2):
                wp_in(p, r, d).wait_recv()

    for d in (2, 1, 3):
        o1(d).start()
    for i in range(4):
        tok(i).start()
    for i in range(4):
        local[i + 1].wait()
    w1[1].out(0).start()
    w1[1].out(1).start()
    w1_across().start()
    local[0].wait()
    w1[0].out(0).start()
    w1[0].out(1).start()
    ACC[...] = jnp.zeros_like(ACC)
    LS[...] = jnp.zeros_like(LS)
    MX[...] = jnp.full(MX.shape, -jnp.inf, F32)
    def o3_send(r):
        o3[r].out(0).start()
        o3[r].out(1).start()
        op(r, 0).start()

    def o2_send():
        local[5].wait()
        for d in (1, 3, 2):
            o1_in(d).wait_recv()
        o2.out(0).start()
        o2.out(1).start()

    def o2_pass_on():
        for k in range(2):
            o2.into(k).wait_recv()
            o2.out(k + 2).start()
            o3_send(3 if k == 0 else 1)

    order = (0, 3, 1, 2)
    w1_near(1)
    for r in order[:3]:
        w2_send(1, r)
    w1_far(1)
    w2_send(1, 2)
    w1_near(0)
    pl.when(c == 0)(o2_send)
    for r in order:
        w2_near(1, r)
    w1_far(0)
    for r in order:
        w2_send(0, r)
    pl.when(c == 1)(o2_send)
    for r in order:
        w2_far(1, r)
    wp_wait(1)
    local[6].wait()
    lane = lax.broadcasted_iota(jnp.int32, (64, HD), 1)
    low64 = lane < 64
    even = lane % 2 == 0

    def normed_turned(raw, gain, cosv, sin_a, sin_b):
        n = raw * lax.rsqrt(jnp.mean(raw * raw, axis=1, keepdims=True) + EPS) * gain
        return n * cosv + (pltpu.roll(n, HD - 1, 1) * sin_a + pltpu.roll(n, 1, 1) * sin_b)

    def turns_of(v):
        turns = []
        for g in range(4):
            row = (ring(z, set_off(v, g // 2)) * 4 + y) * 4 + g
            cosv = jnp.where(low64, cos_ref[pl.ds(row, 1), :], cos_ref[...])
            sinv = jnp.where(low64, sin_ref[pl.ds(row, 1), :], sin_ref[...])
            turns.append((cosv, jnp.where(even, -sinv, 0.0), jnp.where(even, 0.0, sinv)))
        return turns

    def project_q(v):
        gq = gain_ref[0:1, :]
        turns = turns_of(v)
        for j in range(2):
            raw = jnp.zeros((ROWS, ROWS), F32)
            for k in range(8):
                rq = jnp.concatenate([W[k, 2 * j, 0], W[k, 2 * j + 1, 0]], axis=1)
                raw = raw + jnp.dot(
                    X[v, :, k * 256:(k + 1) * 256], rq, preferred_element_type=F32
                )
            for g in range(4):
                sl = slice(g * 64, (g + 1) * 64)
                for b in range(2):
                    S[j, b, sl, 0:HD] = normed_turned(
                        raw[sl, b * HD:(b + 1) * HD], gq, *turns[g]
                    )
            for half in range(2):
                hs = slice(half * 128, (half + 1) * 128)
                for b in range(2):
                    QT[v, 2 * j + b, :, hs] = S[j, b, hs, 0:HD].T.astype(BF)

    def project_kv(v):
        chunk = y * 4 + v
        gk = gain_ref[1:2, :]
        turns = turns_of(v)
        for j in range(2):
            raw = jnp.zeros((ROWS, ROWS), F32)
            for k in range(8):
                rkv = jnp.concatenate(
                    [
                        jnp.concatenate([W[k, b, 1, 0:128], W[k, b, 1, 128:256]], axis=1)
                        for b in (2 * j, 2 * j + 1)
                    ],
                    axis=0,
                )
                raw = raw + lax.dot_general(
                    X[v, :, k * 256:(k + 1) * 256], rkv, (((1,), (1,)), ((), ())),
                    preferred_element_type=F32,
                )
            for g in range(4):
                sl = slice(g * 64, (g + 1) * 64)
                a0 = raw[sl, 0:HD]
                a1 = raw[sl, HD:]
                kk = jnp.where(low64, a0, pltpu.roll(a1, 64, 1))
                KVB[chunk, j, 0, sl, :] = normed_turned(kk, gk, *turns[g]).astype(BF)
                S[j, 2, sl, 0:HD] = jnp.where(low64, pltpu.roll(a0, 64, 1), a1)
            for half in range(2):
                hs = slice(half * 128, (half + 1) * 128)
                KVB[chunk, j, 1, hs, :] = S[j, 2, hs, 0:HD].T.astype(BF)

    def kv_and_send(v):
        project_kv(v)
        for i in (0, 2, 1, 3):
            kvc(v, i).start()

    def kv_pass_on(v):
        for i in (0, 2):
            kvc(v, i, True).wait_recv()
            kvc(v, 4 + i // 2).start()

    def kv_near(v):
        for i in (1, 3):
            kvc(v, i, True).wait_recv()

    def kv_far(v):
        for i in (4, 5):
            kvc(v, i, True).wait_recv()

    cs = HD ** (-0.5) * math.log2(math.e)
    NEG = jnp.full((8, 256), -jnp.inf, F32)

    def run_units(n, unit_of, chunks, finish=None, events=()):
        refs = [ring(y, dy) * 4 + v for dy, v in chunks]

        def scores(u, j, b, m8):
            v, g = unit_of(u)
            s = jnp.dot(KVB[refs[j], g, 0], QT[v, 2 * g + b], preferred_element_type=F32)
            S[b, j] = s
            return jnp.maximum(m8, jnp.max(s.reshape(32, 8, 256), axis=0))

        def unit(u, m8s, more):
            v, g = unit_of(u)
            news = [NEG, NEG]
            for b in range(2):
                t = v * 4 + 2 * g + b
                m_old = MX[t]
                m = jnp.maximum(
                    m_old, jnp.broadcast_to(jnp.max(m8s[b], axis=0, keepdims=True), (8, 256))
                )
                alpha = jnp.exp2((m_old - m) * cs)
                l8 = LS[t] * alpha
                pv = None
                for j in range(len(refs)):
                    p = jnp.exp2((S[b, j].reshape(32, 8, 256) - m[None]) * cs)
                    l8 = l8 + jnp.sum(p, axis=0)
                    vt = jnp.concatenate(
                        [KVB[refs[j], g, 1, 0:128, :], KVB[refs[j], g, 1, 128:256, :]], axis=1
                    )
                    d = jnp.dot(vt, p.reshape(256, 256).astype(BF), preferred_element_type=F32)
                    pv = d if pv is None else pv + d
                    if more:
                        news[b] = scores(u + 1, j, b, news[b])
                acc = (ACC[t].reshape(16, 8, 256) * alpha[None]).reshape(HD, ROWS) + pv
                if finish is None:
                    MX[t] = m
                    LS[t] = l8
                    ACC[t] = acc
                else:
                    o = acc * (1.0 / jnp.sum(l8, axis=0, keepdims=True))
                    AO[v, 2 * g + b] = o.astype(BF).T
            if finish is not None:
                finish(v, g)
            return tuple(news)

        m8s = [NEG, NEG]
        for j in range(len(refs)):
            for b in range(2):
                m8s[b] = scores(0, j, b, m8s[b])

        def step(u, m8s):
            m8s = unit(u, m8s, True)
            for when, event in events:
                pl.when(u == when)(event)
            return m8s

        unit(n - 1, lax.fori_loop(0, n - 1, step, tuple(m8s)), False)

    def finish(v, g):
        @pl.when(v != 3)
        def _():
            @pl.when(v != 0)
            def _():
                at(v, g, 0).start()
                at(v, g, 1).start()

        @pl.when(v == 3)
        def _():
            relay_in(g, 0).start()
            relay_in(g, 1).start()

    def o2_far():
        o2.into(2).wait_recv()
        o2.into(3).wait_recv()
        o3_send(2)

    def o3_pass_on(*rs):
        for r in rs:
            for k in range(2):
                o3[r].into(k).wait_recv()
                o3[r].out(k + 2).start()
                op(r, 3 if k == 0 else 1).start()

    def o3_far(*rs):
        for r in rs:
            o3[r].into(2).wait_recv()
            o3[r].into(3).wait_recv()
            op(r, 2).start()

    def q_step(v, carry):
        project_q(v)
        return carry

    kv_and_send(0)
    for r in order:
        w2_near(0, r)
    o3_send(0)
    for i in range(2):
        tok(i).wait_recv()
        tok(i + 4).start()
    kv_and_send(1)
    o2_pass_on()
    for r in order:
        w2_far(0, r)
    wp_wait(0)
    lax.fori_loop(0, 2, q_step, 0)
    first_two = lambda u: (u // 2, u % 2)
    set_a = ((0, 0), (0, 1))
    set_b = ((0, 2), (1, 0), (3, 0))
    set_d = ((2, 0), (1, 1), (3, 1))
    run_units(4, first_two, set_a)
    kv_pass_on(0)
    kv_near(0)
    tok(2).wait_recv()
    tok(3).wait_recv()
    kv_and_send(2)
    project_q(2)
    run_units(4, first_two, set_b)
    run_units(2, lambda u: (2, u), set_a + set_b)
    o2_far()
    kv_pass_on(1)
    kv_near(1)
    kv_far(0)
    o3_pass_on(0)
    o3_pass_on(3)
    run_units(6, first_two, set_d)
    tok(4).wait_recv()
    tok(5).wait_recv()
    kv_and_send(3)
    project_q(3)
    run_units(2, lambda u: (3, u), set_a + set_b + set_d)
    kv_pass_on(2)
    kv_near(2)
    kv_far(1)

    run_units(
        8, first_two, ((0, 3), (2, 1), (1, 2), (3, 2)),
        events=(
            (0, lambda: o3_pass_on(1, 2)),
            (2, lambda: kv_pass_on(3)),
            (5, lambda: o3_far(0, 3)),
        ),
    )
    kv_far(2)
    kv_near(3)
    kv_far(3)

    def relay(g):
        for half in range(2):
            relay_in(g, half).wait_recv()
            relay_out(g, half).start()

    last = ((2, 2), (1, 3), (3, 3), (2, 3))
    run_units(4, lambda u: (3 - u, 0), last, finish=finish)
    run_units(
        4, lambda u: (3 - u, 1), last, finish=finish,
        events=((0, lambda: o3_far(1, 2)), (1, lambda: relay(0))),
    )
    relay(1)
    def out_terms(n, who):
        zc, yc = n // 2, (n % 2) * 2
        total = None
        for r in who:
            zs = ring(z, r)
            for i in range(2):
                src = AO.at[0] if r == 0 else ATT.at[zs]
                lhs = jnp.concatenate([src[2 * i], src[2 * i + 1]], axis=1)
                cols = [WO[i, zs, yc, zc], WO[i, zs, yc + 1, zc]]
                d = jnp.dot(lhs, jnp.concatenate(cols, axis=1), preferred_element_type=F32)
                total = d if total is None else total + d
        return total

    def own_block(zc, carry):
        for half in range(2):
            OF[2 * zc + half] = out_terms(2 * zc + half, (0,))
        return carry

    def out_copy(zc):
        cols = pl.ds(pl.multiple_of(zc * 512, 512), 512)
        return pltpu.make_async_copy(OB.at[zc], out_ref.at[:, cols], out_s.at[zc])

    def out_block(zc, carry):
        for half in range(2):
            total = OF[2 * zc + half] + out_terms(2 * zc + half, (1, 3, 2))
            OB[zc, :, half * 256:(half + 1) * 256] = total.astype(BF)
        out_copy(zc).start()
        return carry

    for r in range(4):
        for d in range(4):
            op_in(r, d).wait_recv()
    lax.fori_loop(0, 4, own_block, 0)
    for v in range(1, 4):
        for g in range(2):
            for half in range(2):
                at_in(v, g, half).wait_recv()
    lax.fori_loop(0, 4, out_block, 0)
    for i in range(6):
        tok(i).wait_send()
    for d in (1, 2, 3):
        o1(d).wait_send()
    w1[1].out(0).wait_send()
    w1[1].out(1).wait_send()
    w1_across().wait_send()
    for k in range(4):
        for stage in (w1[0], o2, *o3, *w2[0], *w2[1]):
            stage.out(k).wait_send()
        for r in range(4):
            op(r, k).wait_send()
            wp(0, r, k).wait_send()
            wp(1, r, k).wait_send()
    for v in range(4):
        for i in range(6):
            kvc(v, i).wait_send()
    for v in range(1, 4):
        for g in range(2):
            for half in range(2):
                (relay_out if v == 3 else functools.partial(at, v))(g, half).wait_send()
    for g in range(2):
        for half in range(2):
            relay_in(g, half).wait_send()
    for n in range(4):
        out_copy(n).wait()


def on_device(tokens, w_query, w_key, w_value, w_out, qk_gain):
    cos_t, sin_t = rope_tables()
    any_ = pl.BlockSpec(memory_space=pl.ANY)
    vm = pl.BlockSpec(memory_space=pltpu.VMEM)
    dma = pltpu.SemaphoreType.DMA
    pair = lambda *shape: [dma(shape), dma(shape)]
    out = pl.pallas_call(
        kernel,
        out_shape=jax.ShapeDtypeStruct((ROWS, 2048), BF),
        in_specs=[any_, any_, any_, any_, any_, vm, vm, vm],
        out_specs=any_,
        scratch_shapes=[
            pltpu.VMEM((4, ROWS, 2048), BF),
            pltpu.VMEM((8, 4, 2, ROWS, HD), BF),
            pltpu.VMEM((2, 4, 4, 4, ROWS, HD), BF),
            pltpu.VMEM((4, 4, HD, ROWS), BF),
            pltpu.VMEM((16, 2, 2, ROWS, HD), BF),
            pltpu.VMEM((2, 8, ROWS, ROWS), F32),
            pltpu.VMEM((16, HD, ROWS), F32),
            pltpu.VMEM((16, 8, ROWS), F32),
            pltpu.VMEM((16, 8, ROWS), F32),
            pltpu.VMEM((4, 4, ROWS, HD), BF),
            pltpu.VMEM((4, 4, ROWS, HD), BF),
            pltpu.VMEM((2, 4, 128, HD), BF),
            pltpu.VMEM((8, ROWS, 256), F32),
            pltpu.VMEM((4, ROWS, 512), BF),
            dma((7,)),
            *pair(6), *pair(2, 4), *pair(2, 4, 4), *pair(2, 4, 4),
            *pair(3), *pair(4), *pair(4, 4), *pair(4, 4),
            *pair(4, 6), *pair(3, 2, 2), *pair(2, 2), dma((4,)),
        ],
        compiler_params=pltpu.CompilerParams(
            collective_id=0, has_side_effects=True, vmem_limit_bytes=56 * 1024 * 1024
        ),
    )(tokens, w_query, w_key.T, w_value.T, w_out, qk_gain, jnp.asarray(cos_t), jnp.asarray(sin_t))
    return out[None]


def solution(mesh):
    in_specs = (
        P("dp", "sp", None),
        P("dp", "sp"),
        P("dp", "sp"),
        P("dp", "sp"),
        P("dp", "sp"),
        P(),
    )
    out_specs = P("dp", "sp", None)
    return jax.shard_map(
        on_device, mesh=mesh, in_specs=in_specs, out_specs=out_specs, check_vma=False
    )
```

```python
import functools
import math

import jax
import jax.numpy as jnp
import numpy as np
from jax import lax
from jax.experimental import pallas as pl
from jax.experimental.pallas import tpu as pltpu
from jax.sharding import PartitionSpec as P

HQ = 16
KV = 8
HD = 128
GRID_W = 64
ROPE_BASE = 10000.0
EPS = 1e-06
ROWS = 256
BF = jnp.bfloat16
F32 = jnp.float32


def rope_tables():
    quarter = np.arange(0, HD // 2, 2, dtype=np.float32)
    inv_freq = np.float32(ROPE_BASE) ** (-quarter / np.float32(HD // 2))
    angle = np.arange(GRID_W, dtype=np.float32)[:, None] * inv_freq.astype(np.float32)
    angle = np.repeat(angle, 2, axis=1).astype(np.float64)
    angle = np.concatenate([angle, angle], axis=1)
    return np.cos(angle).astype(np.float32), np.sin(angle).astype(np.float32)


class Ring:
    def __init__(self, copy, slot, half, step, send, recv):
        self.copy, self.slot, self.half, self.step = copy, slot, half, step
        self.send, self.recv = send, recv

    def out(self, k):
        if k == 0 or k == 1:
            block = self.slot(0)
        elif k == 2:
            block = self.half(self.slot(3), 0)
        else:
            block = self.half(self.slot(1), 1)
        return self.copy(block, block, self.send(k), self.recv(k), **self.step(1 if k % 2 == 0 else 3))

    def into(self, k):
        far = self.slot(2)
        block = (self.slot(3), self.slot(1), self.half(far, 0), self.half(far, 1))[k]
        return self.copy(block, block, self.send(k), self.recv(k), **self.step(1))


def kernel(
    tok_hbm, wq_hbm, wk_hbm, wv_hbm, wo_hbm, gain_hbm, cos_hbm, sin_hbm,
    out_ref,
    gain_ref, cos_ref, sin_ref,
    X, W, WO, QT, KVB, S, ACC, MX, LS, AO, ATT, RB, OF, OB,
    loc, tok_s, tok_r, w1_s, w1_r, w2_s, w2_r, wp_s, wp_r,
    o1_s, o1_r, o2_s, o2_r, o3_s, o3_r, op_s, op_r,
    kv_s, kv_r, at_s, at_r, rl_s, rl_r, out_s,
):
    sp = lax.axis_index("sp")
    dp = lax.axis_index("dp")
    z, y = sp // 4, sp % 4
    x, c = dp // 2, dp % 2

    def ring(v, d):
        return (v + d + 4) % 4

    def device(dz=0, dy=0, dx=0, other=False):
        return {
            "sp": ring(z, dz) * 4 + ring(y, dy),
            "dp": ring(x, dx) * 2 + ((1 - c) if other else c),
        }

    def to(src, dst, ss, rs, **where):
        return pltpu.make_async_remote_copy(
            src_ref=src, dst_ref=dst, send_sem=ss, recv_sem=rs,
            device_id=device(**where), device_id_type=pl.DeviceIdType.MESH,
        )

    lo, hi = pl.ds(0, 128), pl.ds(128, 128)

    local = [
        (wq_hbm, W.at[dp, y, 0]),
        (wk_hbm.at[:, lo], W.at[dp, y, 1, pl.ds(0, 64)]),
        (wk_hbm.at[:, hi], W.at[dp, y, 1, pl.ds(128, 64)]),
        (wv_hbm.at[:, lo], W.at[dp, y, 1, pl.ds(64, 64)]),
        (wv_hbm.at[:, hi], W.at[dp, y, 1, pl.ds(192, 64)]),
        (wo_hbm, WO.at[c, x, y * (1 - c) + z * c, z * (1 - c) + y * c]),
        (tok_hbm.at[0], X.at[0]),
        (gain_hbm, gain_ref),
        (cos_hbm, cos_ref),
        (sin_hbm, sin_ref),
    ]
    local = [pltpu.make_async_copy(a, b, loc.at[i]) for i, (a, b) in enumerate(local)]
    for one in local:
        one.start()

    barrier = pltpu.get_barrier_semaphore()
    for where in (
        dict(dz=1), dict(dz=3), dict(dz=2), dict(dy=1), dict(dy=3), dict(dy=2), dict(dx=1),
        dict(dx=3), dict(dx=2), dict(other=True),
    ):
        pl.semaphore_signal(
            barrier, inc=1, device_id=device(**where), device_id_type=pl.DeviceIdType.MESH
        )
    pl.semaphore_wait(barrier, 10)

    def tok(i):
        dst = (X.at[1, lo], X.at[1, hi], X.at[2, hi], X.at[2, lo], X.at[3, lo], X.at[3, hi])[i]
        src = (
            tok_hbm.at[0, lo], tok_hbm.at[0, hi], tok_hbm.at[0, hi], tok_hbm.at[0, lo],
            X.at[1, lo], X.at[1, hi],
        )[i]
        return to(src, dst, tok_s.at[i], tok_r.at[i], dz=1 if i % 2 == 0 else 3)

    def set_off(v, half):
        gray = v ^ (v >> 1)
        return gray if half else (4 - gray) % 4

    def wslot(cc, d1, d2, part):
        cc1 = cc * part
        return W.at[
            ring(x, d2 * (1 - cc1) + d1 * cc1) * 2 + cc, ring(y, d1 * (1 - cc1) + d2 * cc1), part
        ]

    first_half = lambda ref, i: ref.at[i]
    row_half = lambda ref, i: ref.at[hi if i else lo]
    w1 = [
        Ring(
            to, lambda d, p=p: wslot(c, d, 0, p), row_half,
            lambda d, p=p: dict(dy=d * (1 - c * p), dx=d * c * p),
            lambda k, p=p: w1_s.at[p, k], lambda k, p=p: w1_r.at[p, k],
        )
        for p in range(2)
    ]
    w2 = [
        [
            Ring(
                to, lambda d, r=r, p=p: wslot(c, r, d, p), row_half,
                lambda d, p=p: dict(dy=d * c * p, dx=d * (1 - c * p)),
                lambda k, r=r, p=p: w2_s.at[p, r, k], lambda k, r=r, p=p: w2_r.at[p, r, k],
            )
            for r in range(4)
        ]
        for p in range(2)
    ]

    def wp(p, r, d):
        b = wslot(c, r, d, p)
        return to(b, b, wp_s.at[p, r, d], wp_r.at[p, r, d], other=True)

    def wp_in(p, r, d):
        b = wslot(1 - c, r, d, p)
        return to(b, b, wp_s.at[p, r, d], wp_r.at[p, r, d], other=True)

    oa, ob, oc = x, y * (1 - c) + z * c, z * (1 - c) + y * c

    def o1(d):
        return to(
            wo_hbm, WO.at[c, oa, ob, oc], o1_s.at[d - 1], o1_r.at[d - 1],
            dz=d * (1 - c), dy=d * c,
        )

    def o1_in(d):
        b = WO.at[c, oa, ob, ring(oc, -d)]
        return to(b, b, o1_s.at[d - 1], o1_r.at[d - 1], dz=1)

    two = lambda ref, i: ref.at[pl.ds(2 * i, 2)]
    o2 = Ring(
        to, lambda d: WO.at[c, oa, ring(ob, d)], two,
        lambda d: dict(dy=d * (1 - c), dz=d * c), lambda k: o2_s.at[k], lambda k: o2_r.at[k],
    )
    o3 = [
        Ring(
            to, lambda d, r=r: WO.at[c, ring(oa, d), ring(ob, r)], two,
            lambda d: dict(dx=d), lambda k, r=r: o3_s.at[r, k], lambda k, r=r: o3_r.at[r, k],
        )
        for r in range(4)
    ]

    def op(r, d):
        b = WO.at[c, ring(oa, d), ring(ob, r)]
        return to(b, b, op_s.at[r, d], op_r.at[r, d], other=True)

    def op_in(r, d):
        b = WO.at[1 - c, ring(oa, d), ring(y * c + z * (1 - c), r)]
        return to(b, b, op_s.at[r, d], op_r.at[r, d], other=True)

    def kvc(v, i, landing=False):
        half = (0, 1, 1, 0, 0, 1)[i]
        from_y = ((3, 3, 1, 1, 2, 2) if landing else (0, 0, 0, 0, 3, 1))[i]
        b = KVB.at[ring(y, from_y) * 4 + v, half]
        return to(b, b, kv_s.at[v, i], kv_r.at[v, i], dy=(1, 1, 3, 3, 1, 3)[i])

    def at(v, g, half):
        rows, heads = hi if half else lo, pl.ds(2 * g, 2)
        return to(
            AO.at[v, heads, rows], ATT.at[z, heads, rows],
            at_s.at[v - 1, g, half], at_r.at[v - 1, g, half], dz=set_off(v, half),
        )

    def at_in(v, g, half):
        b = ATT.at[ring(z, -set_off(v, half)), pl.ds(2 * g, 2), hi if half else lo]
        return to(b, b, at_s.at[v - 1, g, half], at_r.at[v - 1, g, half], dz=1)

    def relay_in(g, half):
        heads = pl.ds(2 * g, 2)
        return to(
            AO.at[3, heads, hi if half else lo], RB.at[half, heads],
            rl_s.at[g, half], rl_r.at[g, half], dz=3 if half else 1,
        )

    def relay_out(g, half):
        heads = pl.ds(2 * g, 2)
        return to(
            RB.at[half, heads], ATT.at[ring(z, 1 if half else 3), heads, hi if half else lo],
            at_s.at[2, g, half], at_r.at[2, g, half], dz=3 if half else 1,
        )

    def w1_near(p):
        for k in range(2):
            w1[p].into(k).wait_recv()
            if p == 0:
                w1[p].out(k + 2).start()

    def w1_far(p):
        if p == 0:
            w1[p].into(2).wait_recv()
            w1[p].into(3).wait_recv()
        else:
            w1_across(True).wait_recv()

    def w1_across(landing=False):
        b = wslot(c, 2 if landing else 0, 0, 1)
        return to(b, b, w1_s.at[1, 2], w1_r.at[1, 2], dy=2 * (1 - c), dx=2 * c)

    def w2_send(p, r):
        w2[p][r].out(0).start()
        w2[p][r].out(1).start()
        wp(p, r, 0).start()

    def w2_near(p, r):
        for k in range(2):
            w2[p][r].into(k).wait_recv()
            w2[p][r].out(k + 2).start()
            wp(p, r, 3 if k == 0 else 1).start()

    def w2_far(p, r):
        w2[p][r].into(2).wait_recv()
        w2[p][r].into(3).wait_recv()
        wp(p, r, 2).start()

    def wp_wait(p):
        for r in (0, 3, 1, 2):
            for d in (0, 3, 1, 2):
                wp_in(p, r, d).wait_recv()

    def o1_send():
        for d in (2, 1, 3):
            o1(d).start()

    pl.when(c == 0)(o1_send)
    for i in range(4):
        tok(i).start()
    for i in range(4):
        local[i + 1].wait()
    w1[1].out(0).start()
    w1[1].out(1).start()
    w1_across().start()
    local[0].wait()
    w1[0].out(0).start()
    w1[0].out(1).start()
    ACC[...] = jnp.zeros_like(ACC)
    LS[...] = jnp.zeros_like(LS)
    MX[...] = jnp.full(MX.shape, -jnp.inf, F32)
    def o3_send(r):
        o3[r].out(0).start()
        o3[r].out(1).start()
        op(r, 0).start()

    def o2_send():
        local[5].wait()
        for d in (1, 3, 2):
            o1_in(d).wait_recv()
        o2.out(0).start()
        o2.out(1).start()

    def o2_pass_on():
        for k in range(2):
            o2.into(k).wait_recv()
            o2.out(k + 2).start()
            o3_send(3 if k == 0 else 1)

    order = (0, 3, 1, 2)
    w1_near(1)
    for r in order[:3]:
        w2_send(1, r)
    w1_far(1)
    w2_send(1, 2)
    w1_near(0)
    pl.when(c == 0)(o2_send)
    for r in order:
        w2_near(1, r)
    w1_far(0)
    for r in order:
        w2_send(0, r)
    pl.when(c == 1)(o1_send)
    for r in order:
        w2_far(1, r)
    wp_wait(1)
    for i in range(6, 10):
        local[i].wait()
    lane = lax.broadcasted_iota(jnp.int32, (64, HD), 1)
    low64 = lane < 64
    even = lane % 2 == 0

    def normed_turned(raw, gain, cosv, sin_a, sin_b):
        n = raw * lax.rsqrt(jnp.mean(raw * raw, axis=1, keepdims=True) + EPS) * gain
        return n * cosv + (pltpu.roll(n, HD - 1, 1) * sin_a + pltpu.roll(n, 1, 1) * sin_b)

    def turns_of(v):
        turns = []
        for g in range(4):
            row = (ring(z, set_off(v, g // 2)) * 4 + y) * 4 + g
            cosv = jnp.where(low64, cos_ref[pl.ds(row, 1), :], cos_ref[...])
            sinv = jnp.where(low64, sin_ref[pl.ds(row, 1), :], sin_ref[...])
            turns.append((cosv, jnp.where(even, -sinv, 0.0), jnp.where(even, 0.0, sinv)))
        return turns

    def project_q(v):
        gq = gain_ref[0:1, :]
        turns = turns_of(v)
        for j in range(2):
            raw = jnp.zeros((ROWS, ROWS), F32)
            for k in range(8):
                rq = jnp.concatenate([W[k, 2 * j, 0], W[k, 2 * j + 1, 0]], axis=1)
                raw = raw + jnp.dot(
                    X[v, :, k * 256:(k + 1) * 256], rq, preferred_element_type=F32
                )
            for g in range(4):
                sl = slice(g * 64, (g + 1) * 64)
                for b in range(2):
                    S[j, b, sl, 0:HD] = normed_turned(
                        raw[sl, b * HD:(b + 1) * HD], gq, *turns[g]
                    )
            for half in range(2):
                hs = slice(half * 128, (half + 1) * 128)
                for b in range(2):
                    QT[v, 2 * j + b, :, hs] = S[j, b, hs, 0:HD].T.astype(BF)

    def project_kv(v):
        chunk = y * 4 + v
        gk = gain_ref[1:2, :]
        turns = turns_of(v)
        for j in range(2):
            raw = jnp.zeros((ROWS, ROWS), F32)
            for k in range(8):
                rkv = jnp.concatenate(
                    [
                        jnp.concatenate([W[k, b, 1, 0:128], W[k, b, 1, 128:256]], axis=1)
                        for b in (2 * j, 2 * j + 1)
                    ],
                    axis=0,
                )
                raw = raw + lax.dot_general(
                    X[v, :, k * 256:(k + 1) * 256], rkv, (((1,), (1,)), ((), ())),
                    preferred_element_type=F32,
                )
            for g in range(4):
                sl = slice(g * 64, (g + 1) * 64)
                a0 = raw[sl, 0:HD]
                a1 = raw[sl, HD:]
                kk = jnp.where(low64, a0, pltpu.roll(a1, 64, 1))
                KVB[chunk, j, 0, sl, :] = normed_turned(kk, gk, *turns[g]).astype(BF)
                S[j, 2, sl, 0:HD] = jnp.where(low64, pltpu.roll(a0, 64, 1), a1)
            for half in range(2):
                hs = slice(half * 128, (half + 1) * 128)
                KVB[chunk, j, 1, hs, :] = S[j, 2, hs, 0:HD].T.astype(BF)

    def kv_and_send(v):
        project_kv(v)
        for i in (0, 2, 1, 3):
            kvc(v, i).start()

    def kv_pass_on(v):
        for i in (0, 2):
            kvc(v, i, True).wait_recv()
            kvc(v, 4 + i // 2).start()

    def kv_near(v):
        for i in (1, 3):
            kvc(v, i, True).wait_recv()

    def kv_far(v):
        for i in (4, 5):
            kvc(v, i, True).wait_recv()

    cs = HD ** (-0.5) * math.log2(math.e)
    NEG = jnp.full((8, 256), -jnp.inf, F32)

    def run_units(n, unit_of, chunks, finish=None, events=()):
        refs = [ring(y, dy) * 4 + v for dy, v in chunks]

        def scores(u, j, b, m8):
            v, g = unit_of(u)
            s = jnp.dot(KVB[refs[j], g, 0], QT[v, 2 * g + b], preferred_element_type=F32)
            S[b, j] = s
            return jnp.maximum(m8, jnp.max(s.reshape(32, 8, 256), axis=0))

        def unit(u, m8s, more):
            v, g = unit_of(u)
            news = [NEG, NEG]
            for b in range(2):
                t = v * 4 + 2 * g + b
                m_old = MX[t]
                m = jnp.maximum(
                    m_old, jnp.broadcast_to(jnp.max(m8s[b], axis=0, keepdims=True), (8, 256))
                )
                alpha = jnp.exp2((m_old - m) * cs)
                l8 = LS[t] * alpha
                pv = None
                for j in range(len(refs)):
                    p = jnp.exp2((S[b, j].reshape(32, 8, 256) - m[None]) * cs)
                    l8 = l8 + jnp.sum(p, axis=0)
                    vt = jnp.concatenate(
                        [KVB[refs[j], g, 1, 0:128, :], KVB[refs[j], g, 1, 128:256, :]], axis=1
                    )
                    d = jnp.dot(vt, p.reshape(256, 256).astype(BF), preferred_element_type=F32)
                    pv = d if pv is None else pv + d
                    if more:
                        news[b] = scores(u + 1, j, b, news[b])
                acc = (ACC[t].reshape(16, 8, 256) * alpha[None]).reshape(HD, ROWS) + pv
                if finish is None:
                    MX[t] = m
                    LS[t] = l8
                    ACC[t] = acc
                else:
                    o = acc * (1.0 / jnp.sum(l8, axis=0, keepdims=True))
                    AO[v, 2 * g + b] = o.astype(BF).T
            if finish is not None:
                finish(v, g)
            return tuple(news)

        m8s = [NEG, NEG]
        for j in range(len(refs)):
            for b in range(2):
                m8s[b] = scores(0, j, b, m8s[b])

        def step(u, m8s):
            m8s = unit(u, m8s, True)
            for when, event in events:
                pl.when(u == when)(event)
            return m8s

        unit(n - 1, lax.fori_loop(0, n - 1, step, tuple(m8s)), False)

    def finish(v, g):
        @pl.when(v != 3)
        def _():
            @pl.when(v != 0)
            def _():
                at(v, g, 0).start()
                at(v, g, 1).start()

        @pl.when(v == 3)
        def _():
            relay_in(g, 0).start()
            relay_in(g, 1).start()

    def o2_far():
        o2.into(2).wait_recv()
        o2.into(3).wait_recv()
        o3_send(2)

    def o3_pass_on(*rs):
        for r in rs:
            for k in range(2):
                o3[r].into(k).wait_recv()
                o3[r].out(k + 2).start()
                op(r, 3 if k == 0 else 1).start()

    def o3_far(*rs):
        for r in rs:
            o3[r].into(2).wait_recv()
            o3[r].into(3).wait_recv()
            op(r, 2).start()

    def q_step(v, carry):
        project_q(v)
        return carry

    kv_and_send(0)
    for r in order:
        w2_near(0, r)
    pl.when(c == 0)(lambda: o3_send(0))
    for i in range(2):
        tok(i).wait_recv()
        tok(i + 4).start()

    @pl.when(c == 1)
    def _():
        o2_send()
        o3_send(0)
    kv_and_send(1)
    pl.when(c == 0)(o2_pass_on)
    for r in order:
        w2_far(0, r)
    wp_wait(0)
    lax.fori_loop(0, 2, q_step, 0)
    first_two = lambda u: (u // 2, u % 2)
    set_a = ((0, 0), (0, 1))
    set_b = ((0, 2), (1, 0), (3, 0))
    set_d = ((2, 0), (1, 1), (3, 1))
    run_units(4, first_two, set_a)
    kv_pass_on(0)
    kv_near(0)
    tok(2).wait_recv()
    tok(3).wait_recv()
    kv_and_send(2)
    project_q(2)
    run_units(4, first_two, set_b)
    run_units(2, lambda u: (2, u), set_a + set_b)
    pl.when(c == 0)(o2_far)
    kv_pass_on(1)
    kv_near(1)
    kv_far(0)
    o3_pass_on(0)
    pl.when(c == 0)(lambda: o3_pass_on(3))
    run_units(6, first_two, set_d)
    tok(4).wait_recv()
    tok(5).wait_recv()
    kv_and_send(3)
    project_q(3)
    pl.when(c == 1)(o2_pass_on)

    def on_core(core, event, *rs):
        return lambda: pl.when(c == core)(lambda: event(*rs))

    run_units(2, lambda u: (3, u), set_a + set_b + set_d)
    kv_pass_on(2)
    kv_near(2)
    kv_far(1)

    run_units(
        8, first_two, ((0, 3), (2, 1), (1, 2), (3, 2)),
        events=(
            (0, on_core(0, o3_pass_on, 1, 2)),
            (0, on_core(1, o2_far)),
            (2, lambda: kv_pass_on(3)),
            (5, lambda: o3_far(0)),
            (5, on_core(0, o3_far, 3)),
            (6, on_core(1, o3_pass_on, 3, 1)),
        ),
    )
    kv_far(2)
    kv_near(3)
    kv_far(3)

    def relay(g):
        for half in range(2):
            relay_in(g, half).wait_recv()
            relay_out(g, half).start()

    last = ((2, 2), (1, 3), (3, 3), (2, 3))
    run_units(4, lambda u: (3 - u, 0), last, finish=finish)
    run_units(
        4, lambda u: (3 - u, 1), last, finish=finish,
        events=(
            (0, on_core(0, o3_far, 1, 2)),
            (0, on_core(1, o3_far, 3, 1)),
            (1, on_core(1, o3_pass_on, 2)),
            (1, lambda: relay(0)),
        ),
    )
    relay(1)
    on_core(1, o3_far, 2)()
    def out_terms(n, who):
        zc, yc = n // 2, (n % 2) * 2
        total = None
        for r in who:
            zs = ring(z, r)
            for i in range(2):
                src = AO.at[0] if r == 0 else ATT.at[zs]
                lhs = jnp.concatenate([src[2 * i], src[2 * i + 1]], axis=1)
                if i == 0:
                    cols = [WO[0, zs, yc, zc], WO[0, zs, yc + 1, zc]]
                else:
                    cols = [WO[1, zs, zc, yc], WO[1, zs, zc, yc + 1]]
                d = jnp.dot(lhs, jnp.concatenate(cols, axis=1), preferred_element_type=F32)
                total = d if total is None else total + d
        return total

    def own_block(zc, carry):
        for half in range(2):
            OF[2 * zc + half] = out_terms(2 * zc + half, (0,))
        return carry

    def out_copy(zc):
        cols = pl.ds(pl.multiple_of(zc * 512, 512), 512)
        return pltpu.make_async_copy(OB.at[zc], out_ref.at[:, cols], out_s.at[zc])

    def out_block(zc, carry):
        for half in range(2):
            total = OF[2 * zc + half] + out_terms(2 * zc + half, (1, 3, 2))
            OB[zc, :, half * 256:(half + 1) * 256] = total.astype(BF)
        out_copy(zc).start()
        return carry

    for r in range(4):
        for d in range(4):
            op_in(r, d).wait_recv()
    lax.fori_loop(0, 4, own_block, 0)
    for v in range(1, 4):
        for g in range(2):
            for half in range(2):
                at_in(v, g, half).wait_recv()
    lax.fori_loop(0, 4, out_block, 0)
    for i in range(6):
        tok(i).wait_send()
    for d in (1, 2, 3):
        o1(d).wait_send()
    w1[1].out(0).wait_send()
    w1[1].out(1).wait_send()
    w1_across().wait_send()
    for k in range(4):
        for stage in (w1[0], o2, *o3, *w2[0], *w2[1]):
            stage.out(k).wait_send()
        for r in range(4):
            op(r, k).wait_send()
            wp(0, r, k).wait_send()
            wp(1, r, k).wait_send()
    for v in range(4):
        for i in range(6):
            kvc(v, i).wait_send()
    for v in range(1, 4):
        for g in range(2):
            for half in range(2):
                (relay_out if v == 3 else functools.partial(at, v))(g, half).wait_send()
    for g in range(2):
        for half in range(2):
            relay_in(g, half).wait_send()
    for n in range(4):
        out_copy(n).wait()


def on_device(tokens, w_query, w_key, w_value, w_out, qk_gain):
    cos_t, sin_t = rope_tables()
    any_ = pl.BlockSpec(memory_space=pl.ANY)
    vm = pl.BlockSpec(memory_space=pltpu.VMEM)
    dma = pltpu.SemaphoreType.DMA
    pair = lambda *shape: [dma(shape), dma(shape)]
    out = pl.pallas_call(
        kernel,
        out_shape=jax.ShapeDtypeStruct((ROWS, 2048), BF),
        in_specs=[any_] * 8,
        out_specs=any_,
        scratch_shapes=[
            pltpu.VMEM((2, HD), F32),
            pltpu.VMEM((GRID_W, HD), F32),
            pltpu.VMEM((GRID_W, HD), F32),
            pltpu.VMEM((4, ROWS, 2048), BF),
            pltpu.VMEM((8, 4, 2, ROWS, HD), BF),
            pltpu.VMEM((2, 4, 4, 4, ROWS, HD), BF),
            pltpu.VMEM((4, 4, HD, ROWS), BF),
            pltpu.VMEM((16, 2, 2, ROWS, HD), BF),
            pltpu.VMEM((2, 8, ROWS, ROWS), F32),
            pltpu.VMEM((16, HD, ROWS), F32),
            pltpu.VMEM((16, 8, ROWS), F32),
            pltpu.VMEM((16, 8, ROWS), F32),
            pltpu.VMEM((4, 4, ROWS, HD), BF),
            pltpu.VMEM((4, 4, ROWS, HD), BF),
            pltpu.VMEM((2, 4, 128, HD), BF),
            pltpu.VMEM((8, ROWS, 256), F32),
            pltpu.VMEM((4, ROWS, 512), BF),
            dma((10,)),
            *pair(6), *pair(2, 4), *pair(2, 4, 4), *pair(2, 4, 4),
            *pair(3), *pair(4), *pair(4, 4), *pair(4, 4),
            *pair(4, 6), *pair(3, 2, 2), *pair(2, 2), dma((4,)),
        ],
        compiler_params=pltpu.CompilerParams(
            collective_id=0, has_side_effects=True, vmem_limit_bytes=56 * 1024 * 1024
        ),
    )(tokens, w_query, w_key.T, w_value.T, w_out, qk_gain, jnp.asarray(cos_t), jnp.asarray(sin_t))
    return out[None]


def solution(mesh):
    in_specs = (
        P("dp", "sp", None),
        P("dp", "sp"),
        P("dp", "sp"),
        P("dp", "sp"),
        P("dp", "sp"),
        P(),
    )
    out_specs = P("dp", "sp", None)
    return jax.shard_map(
        on_device, mesh=mesh, in_specs=in_specs, out_specs=out_specs, check_vma=False
    )
```

```python
import functools
import math

import jax
import jax.numpy as jnp
import numpy as np
from jax import lax
from jax.experimental import pallas as pl
from jax.experimental.pallas import tpu as pltpu
from jax.sharding import PartitionSpec as P

HQ = 16
KV = 8
HD = 128
GRID_W = 64
ROPE_BASE = 10000.0
EPS = 1e-06
ROWS = 256
BF = jnp.bfloat16
F32 = jnp.float32


def rope_tables():
    quarter = np.arange(0, HD // 2, 2, dtype=np.float32)
    inv_freq = np.float32(ROPE_BASE) ** (-quarter / np.float32(HD // 2))
    angle = np.arange(GRID_W, dtype=np.float32)[:, None] * inv_freq.astype(np.float32)
    angle = np.repeat(angle, 2, axis=1).astype(np.float64)
    angle = np.concatenate([angle, angle], axis=1)
    return np.cos(angle).astype(np.float32), np.sin(angle).astype(np.float32)


class Ring:
    def __init__(self, copy, slot, half, step, send, recv):
        self.copy, self.slot, self.half, self.step = copy, slot, half, step
        self.send, self.recv = send, recv

    def out(self, k):
        if k == 0 or k == 1:
            block = self.slot(0)
        elif k == 2:
            block = self.half(self.slot(3), 0)
        else:
            block = self.half(self.slot(1), 1)
        return self.copy(block, block, self.send(k), self.recv(k), **self.step(1 if k % 2 == 0 else 3))

    def into(self, k):
        far = self.slot(2)
        block = (self.slot(3), self.slot(1), self.half(far, 0), self.half(far, 1))[k]
        return self.copy(block, block, self.send(k), self.recv(k), **self.step(1))


def kernel(
    tok_hbm, wq_hbm, wk_hbm, wv_hbm, wo_hbm, gain_hbm, cos_hbm, sin_hbm,
    out_ref,
    gain_ref, cos_ref, sin_ref,
    X, W, WO, QT, KVB, S, ACC, MX, LS, AO, ATT, RB, OF, OB,
    loc, tok_s, tok_r, w1_s, w1_r, w2_s, w2_r, wp_s, wp_r,
    o1_s, o1_r, o2_s, o2_r, o3_s, o3_r, op_s, op_r,
    kv_s, kv_r, at_s, at_r, rl_s, rl_r, out_s,
):
    sp = lax.axis_index("sp")
    dp = lax.axis_index("dp")
    z, y = sp // 4, sp % 4
    x, c = dp // 2, dp % 2

    def ring(v, d):
        return (v + d + 4) % 4

    def device(dz=0, dy=0, dx=0, other=False):
        return {
            "sp": ring(z, dz) * 4 + ring(y, dy),
            "dp": ring(x, dx) * 2 + ((1 - c) if other else c),
        }

    def to(src, dst, ss, rs, **where):
        return pltpu.make_async_remote_copy(
            src_ref=src, dst_ref=dst, send_sem=ss, recv_sem=rs,
            device_id=device(**where), device_id_type=pl.DeviceIdType.MESH,
        )

    lo, hi = pl.ds(0, 128), pl.ds(128, 128)

    local = [
        (wq_hbm, W.at[dp, y, 0]),
        (wk_hbm.at[:, lo], W.at[dp, y, 1, pl.ds(0, 64)]),
        (wk_hbm.at[:, hi], W.at[dp, y, 1, pl.ds(128, 64)]),
        (wv_hbm.at[:, lo], W.at[dp, y, 1, pl.ds(64, 64)]),
        (wv_hbm.at[:, hi], W.at[dp, y, 1, pl.ds(192, 64)]),
        (wo_hbm, WO.at[c, x, y * (1 - c) + z * c, z * (1 - c) + y * c]),
        (tok_hbm.at[0], X.at[0]),
        (gain_hbm, gain_ref),
        (cos_hbm, cos_ref),
        (sin_hbm, sin_ref),
    ]
    local = [pltpu.make_async_copy(a, b, loc.at[i]) for i, (a, b) in enumerate(local)]
    for one in local:
        one.start()

    barrier = pltpu.get_barrier_semaphore()
    for where in (
        dict(dz=1), dict(dz=3), dict(dz=2), dict(dy=1), dict(dy=3), dict(dy=2), dict(dx=1),
        dict(dx=3), dict(dx=2), dict(other=True),
    ):
        pl.semaphore_signal(
            barrier, inc=1, device_id=device(**where), device_id_type=pl.DeviceIdType.MESH
        )
    pl.semaphore_wait(barrier, 10)

    def tok(i):
        dst = (X.at[1, lo], X.at[1, hi], X.at[2, hi], X.at[2, lo], X.at[3, lo], X.at[3, hi])[i]
        src = (
            tok_hbm.at[0, lo], tok_hbm.at[0, hi], tok_hbm.at[0, hi], tok_hbm.at[0, lo],
            X.at[1, lo], X.at[1, hi],
        )[i]
        return to(src, dst, tok_s.at[i], tok_r.at[i], dz=1 if i % 2 == 0 else 3)

    def set_off(v, half):
        gray = v ^ (v >> 1)
        return gray if half else (4 - gray) % 4

    def wslot(cc, d1, d2, part):
        cc1 = cc * part
        return W.at[
            ring(x, d2 * (1 - cc1) + d1 * cc1) * 2 + cc, ring(y, d1 * (1 - cc1) + d2 * cc1), part
        ]

    first_half = lambda ref, i: ref.at[i]
    row_half = lambda ref, i: ref.at[hi if i else lo]
    w1 = [
        Ring(
            to, lambda d, p=p: wslot(c, d, 0, p), row_half,
            lambda d, p=p: dict(dy=d * (1 - c * p), dx=d * c * p),
            lambda k, p=p: w1_s.at[p, k], lambda k, p=p: w1_r.at[p, k],
        )
        for p in range(2)
    ]
    w2 = [
        [
            Ring(
                to, lambda d, r=r, p=p: wslot(c, r, d, p), row_half,
                lambda d, p=p: dict(dy=d * c * p, dx=d * (1 - c * p)),
                lambda k, r=r, p=p: w2_s.at[p, r, k], lambda k, r=r, p=p: w2_r.at[p, r, k],
            )
            for r in range(4)
        ]
        for p in range(2)
    ]

    def wp(p, r, d):
        b = wslot(c, r, d, p)
        return to(b, b, wp_s.at[p, r, d], wp_r.at[p, r, d], other=True)

    def wp_in(p, r, d):
        b = wslot(1 - c, r, d, p)
        return to(b, b, wp_s.at[p, r, d], wp_r.at[p, r, d], other=True)

    oa, ob, oc = x, y * (1 - c) + z * c, z * (1 - c) + y * c

    def o1(d):
        return to(
            wo_hbm, WO.at[c, oa, ob, oc], o1_s.at[d - 1], o1_r.at[d - 1],
            dz=d * (1 - c), dy=d * c,
        )

    def o1_in(d):
        b = WO.at[c, oa, ob, ring(oc, -d)]
        return to(b, b, o1_s.at[d - 1], o1_r.at[d - 1], dz=1)

    two = lambda ref, i: ref.at[pl.ds(2 * i, 2)]
    o2 = Ring(
        to, lambda d: WO.at[c, oa, ring(ob, d)], two,
        lambda d: dict(dy=d * (1 - c), dz=d * c), lambda k: o2_s.at[k], lambda k: o2_r.at[k],
    )
    o3 = [
        Ring(
            to, lambda d, r=r: WO.at[c, ring(oa, d), ring(ob, r)], two,
            lambda d: dict(dx=d), lambda k, r=r: o3_s.at[r, k], lambda k, r=r: o3_r.at[r, k],
        )
        for r in range(4)
    ]

    def op(r, d):
        b = WO.at[c, ring(oa, d), ring(ob, r)]
        return to(b, b, op_s.at[r, d], op_r.at[r, d], other=True)

    def op_in(r, d):
        b = WO.at[1 - c, ring(oa, d), ring(y * c + z * (1 - c), r)]
        return to(b, b, op_s.at[r, d], op_r.at[r, d], other=True)

    def kvc(v, i, landing=False):
        half = (0, 1, 1, 0, 0, 1)[i]
        from_y = ((3, 3, 1, 1, 2, 2) if landing else (0, 0, 0, 0, 3, 1))[i]
        b = KVB.at[ring(y, from_y) * 4 + v, half]
        return to(b, b, kv_s.at[v, i], kv_r.at[v, i], dy=(1, 1, 3, 3, 1, 3)[i])

    def at(v, g, half):
        rows, heads = hi if half else lo, pl.ds(2 * g, 2)
        return to(
            AO.at[v, heads, rows], ATT.at[z, heads, rows],
            at_s.at[v - 1, g, half], at_r.at[v - 1, g, half], dz=set_off(v, half),
        )

    def at_in(v, g, half):
        b = ATT.at[ring(z, -set_off(v, half)), pl.ds(2 * g, 2), hi if half else lo]
        return to(b, b, at_s.at[v - 1, g, half], at_r.at[v - 1, g, half], dz=1)

    def relay_in(g, half):
        heads = pl.ds(2 * g, 2)
        return to(
            AO.at[3, heads, hi if half else lo], RB.at[half, heads],
            rl_s.at[g, half], rl_r.at[g, half], dz=3 if half else 1,
        )

    def relay_out(g, half):
        heads = pl.ds(2 * g, 2)
        return to(
            RB.at[half, heads], ATT.at[ring(z, 1 if half else 3), heads, hi if half else lo],
            at_s.at[2, g, half], at_r.at[2, g, half], dz=3 if half else 1,
        )

    def w1_near(p):
        for k in range(2):
            w1[p].into(k).wait_recv()
            if p == 0:
                w1[p].out(k + 2).start()

    def w1_far(p):
        if p == 0:
            w1[p].into(2).wait_recv()
            w1[p].into(3).wait_recv()
        else:
            w1_across(True).wait_recv()

    def w1_across(landing=False):
        b = wslot(c, 2 if landing else 0, 0, 1)
        return to(b, b, w1_s.at[1, 2], w1_r.at[1, 2], dy=2 * (1 - c), dx=2 * c)

    def w2_send(p, r):
        w2[p][r].out(0).start()
        w2[p][r].out(1).start()
        wp(p, r, 0).start()

    def w2_near(p, r):
        for k in range(2):
            w2[p][r].into(k).wait_recv()
            w2[p][r].out(k + 2).start()
            wp(p, r, 3 if k == 0 else 1).start()

    def w2_far(p, r):
        w2[p][r].into(2).wait_recv()
        w2[p][r].into(3).wait_recv()
        wp(p, r, 2).start()

    def wp_wait(p):
        for r in (0, 3, 1, 2):
            for d in (0, 3, 1, 2):
                wp_in(p, r, d).wait_recv()

    def o1_send():
        for d in (2, 1, 3):
            o1(d).start()

    pl.when(c == 0)(o1_send)
    for i in range(4):
        tok(i).start()
    for i in range(4):
        local[i + 1].wait()
    w1[1].out(0).start()
    w1[1].out(1).start()
    w1_across().start()
    local[0].wait()
    w1[0].out(0).start()
    w1[0].out(1).start()
    ACC[...] = jnp.zeros_like(ACC)
    LS[...] = jnp.zeros_like(LS)
    MX[...] = jnp.full(MX.shape, -jnp.inf, F32)
    def o3_send(r):
        o3[r].out(0).start()
        o3[r].out(1).start()
        op(r, 0).start()

    def o2_send():
        local[5].wait()
        for d in (1, 3, 2):
            o1_in(d).wait_recv()
        o2.out(0).start()
        o2.out(1).start()

    def o2_pass_on():
        for k in range(2):
            o2.into(k).wait_recv()
            o2.out(k + 2).start()
            o3_send(3 if k == 0 else 1)

    order = (0, 3, 1, 2)
    w1_near(1)
    for r in order[:3]:
        w2_send(1, r)
    w1_far(1)
    w2_send(1, 2)
    w1_near(0)
    pl.when(c == 0)(o2_send)
    for r in order:
        w2_near(1, r)
    w1_far(0)
    for r in order:
        w2_send(0, r)
    pl.when(c == 1)(o1_send)
    for r in order:
        w2_far(1, r)
    wp_wait(1)
    for i in range(6, 10):
        local[i].wait()
    lane = lax.broadcasted_iota(jnp.int32, (64, HD), 1)
    low64 = lane < 64
    even = lane % 2 == 0

    def normed_turned(raw, gain, cosv, sin_a, sin_b):
        n = raw * lax.rsqrt(jnp.mean(raw * raw, axis=1, keepdims=True) + EPS) * gain
        return n * cosv + (pltpu.roll(n, HD - 1, 1) * sin_a + pltpu.roll(n, 1, 1) * sin_b)

    def turns_of(v):
        turns = []
        for g in range(4):
            row = (ring(z, set_off(v, g // 2)) * 4 + y) * 4 + g
            cosv = jnp.where(low64, cos_ref[pl.ds(row, 1), :], cos_ref[...])
            sinv = jnp.where(low64, sin_ref[pl.ds(row, 1), :], sin_ref[...])
            turns.append((cosv, jnp.where(even, -sinv, 0.0), jnp.where(even, 0.0, sinv)))
        return turns

    def project_q(v):
        gq = gain_ref[0:1, :]
        turns = turns_of(v)
        for j in range(2):
            raw = jnp.zeros((ROWS, ROWS), F32)
            for k in range(8):
                rq = jnp.concatenate([W[k, 2 * j, 0], W[k, 2 * j + 1, 0]], axis=1)
                raw = raw + jnp.dot(
                    X[v, :, k * 256:(k + 1) * 256], rq, preferred_element_type=F32
                )
            for g in range(4):
                sl = slice(g * 64, (g + 1) * 64)
                for b in range(2):
                    S[j, b, sl, 0:HD] = normed_turned(
                        raw[sl, b * HD:(b + 1) * HD], gq, *turns[g]
                    )
            for half in range(2):
                hs = slice(half * 128, (half + 1) * 128)
                for b in range(2):
                    QT[v, 2 * j + b, :, hs] = S[j, b, hs, 0:HD].T.astype(BF)

    def project_kv(v):
        chunk = y * 4 + v
        gk = gain_ref[1:2, :]
        turns = turns_of(v)
        for j in range(2):
            raw = jnp.zeros((ROWS, ROWS), F32)
            for k in range(8):
                rkv = jnp.concatenate(
                    [
                        jnp.concatenate([W[k, b, 1, 0:128], W[k, b, 1, 128:256]], axis=1)
                        for b in (2 * j, 2 * j + 1)
                    ],
                    axis=0,
                )
                raw = raw + lax.dot_general(
                    X[v, :, k * 256:(k + 1) * 256], rkv, (((1,), (1,)), ((), ())),
                    preferred_element_type=F32,
                )
            for g in range(4):
                sl = slice(g * 64, (g + 1) * 64)
                a0 = raw[sl, 0:HD]
                a1 = raw[sl, HD:]
                kk = jnp.where(low64, a0, pltpu.roll(a1, 64, 1))
                KVB[chunk, j, 0, sl, :] = normed_turned(kk, gk, *turns[g]).astype(BF)
                S[j, 2, sl, 0:HD] = jnp.where(low64, pltpu.roll(a0, 64, 1), a1)
            for half in range(2):
                hs = slice(half * 128, (half + 1) * 128)
                KVB[chunk, j, 1, hs, :] = S[j, 2, hs, 0:HD].T.astype(BF)

    def kv_and_send(v):
        project_kv(v)
        for i in (0, 2, 1, 3):
            kvc(v, i).start()

    def kv_pass_on(v):
        for i in (0, 2):
            kvc(v, i, True).wait_recv()
            kvc(v, 4 + i // 2).start()

    def kv_near(v):
        for i in (1, 3):
            kvc(v, i, True).wait_recv()

    def kv_far(v):
        for i in (4, 5):
            kvc(v, i, True).wait_recv()

    cs = HD ** (-0.5) * math.log2(math.e)
    NEG = jnp.full((8, 256), -jnp.inf, F32)

    def run_units(n, unit_of, chunks, finish=None, events=()):
        refs = [ring(y, dy) * 4 + v for dy, v in chunks]

        def scores(u, j, b, m8):
            v, g = unit_of(u)
            s = jnp.dot(KVB[refs[j], g, 0], QT[v, 2 * g + b], preferred_element_type=F32)
            S[b, j] = s
            return jnp.maximum(m8, jnp.max(s.reshape(32, 8, 256), axis=0))

        def unit(u, m8s, more):
            v, g = unit_of(u)
            news = [NEG, NEG]
            for b in range(2):
                t = v * 4 + 2 * g + b
                m_old = MX[t]
                m = jnp.maximum(
                    m_old, jnp.broadcast_to(jnp.max(m8s[b], axis=0, keepdims=True), (8, 256))
                )
                alpha = jnp.exp2((m_old - m) * cs)
                l8 = LS[t] * alpha
                pv = None
                for j in range(len(refs)):
                    p = jnp.exp2((S[b, j].reshape(32, 8, 256) - m[None]) * cs)
                    l8 = l8 + jnp.sum(p, axis=0)
                    vt = jnp.concatenate(
                        [KVB[refs[j], g, 1, 0:128, :], KVB[refs[j], g, 1, 128:256, :]], axis=1
                    )
                    d = jnp.dot(vt, p.reshape(256, 256).astype(BF), preferred_element_type=F32)
                    pv = d if pv is None else pv + d
                    if more:
                        news[b] = scores(u + 1, j, b, news[b])
                acc = (ACC[t].reshape(16, 8, 256) * alpha[None]).reshape(HD, ROWS) + pv
                if finish is None:
                    MX[t] = m
                    LS[t] = l8
                    ACC[t] = acc
                else:
                    o = acc * (1.0 / jnp.sum(l8, axis=0, keepdims=True))
                    AO[v, 2 * g + b] = o.astype(BF).T
            if finish is not None:
                finish(v, g)
            return tuple(news)

        m8s = [NEG, NEG]
        for j in range(len(refs)):
            for b in range(2):
                m8s[b] = scores(0, j, b, m8s[b])

        def step(u, m8s):
            m8s = unit(u, m8s, True)
            for when, event in events:
                pl.when(u == when)(event)
            return m8s

        unit(n - 1, lax.fori_loop(0, n - 1, step, tuple(m8s)), False)

    def finish(v, g):
        @pl.when(v != 3)
        def _():
            @pl.when(v != 0)
            def _():
                at(v, g, 0).start()
                at(v, g, 1).start()

        @pl.when(v == 3)
        def _():
            relay_in(g, 0).start()
            relay_in(g, 1).start()

    def o2_far():
        o2.into(2).wait_recv()
        o2.into(3).wait_recv()
        o3_send(2)

    def o3_pass_on(*rs):
        for r in rs:
            for k in range(2):
                o3[r].into(k).wait_recv()
                o3[r].out(k + 2).start()
                op(r, 3 if k == 0 else 1).start()

    def o3_far(*rs):
        for r in rs:
            o3[r].into(2).wait_recv()
            o3[r].into(3).wait_recv()
            op(r, 2).start()

    def q_step(v, carry):
        project_q(v)
        return carry

    kv_and_send(0)
    for r in order:
        w2_near(0, r)
    pl.when(c == 0)(lambda: o3_send(0))
    for i in range(2):
        tok(i).wait_recv()
        tok(i + 4).start()

    @pl.when(c == 1)
    def _():
        o2_send()
        o3_send(0)
    kv_and_send(1)
    pl.when(c == 0)(o2_pass_on)
    for r in order:
        w2_far(0, r)
    wp_wait(0)
    lax.fori_loop(0, 2, q_step, 0)
    first_two = lambda u: (u // 2, u % 2)
    set_a = ((0, 0), (0, 1))
    set_b = ((0, 2), (1, 0), (3, 0))
    set_d = ((2, 0), (1, 1), (3, 1))
    run_units(4, first_two, set_a)
    kv_pass_on(0)
    kv_near(0)
    tok(2).wait_recv()
    tok(3).wait_recv()
    kv_and_send(2)
    project_q(2)
    run_units(4, first_two, set_b)
    run_units(2, lambda u: (2, u), set_a + set_b)
    pl.when(c == 0)(o2_far)
    kv_pass_on(1)
    kv_near(1)
    kv_far(0)
    o3_pass_on(0)
    pl.when(c == 0)(lambda: o3_pass_on(3))
    run_units(6, first_two, set_d)
    tok(4).wait_recv()
    tok(5).wait_recv()
    kv_and_send(3)
    pl.when(c == 1)(o2_pass_on)
    project_q(3)

    def on_core(core, event, *rs):
        return lambda: pl.when(c == core)(lambda: event(*rs))

    run_units(2, lambda u: (3, u), set_a + set_b + set_d)
    kv_pass_on(2)
    kv_near(2)
    kv_far(1)

    run_units(
        8, first_two, ((0, 3), (2, 1), (1, 2), (3, 2)),
        events=(
            (0, on_core(0, o3_pass_on, 1, 2)),
            (0, on_core(1, o2_far)),
            (2, lambda: kv_pass_on(3)),
            (5, lambda: o3_far(0)),
            (5, on_core(0, o3_far, 3)),
            (6, on_core(1, o3_pass_on, 3, 1)),
        ),
    )
    kv_far(2)
    kv_near(3)
    kv_far(3)

    def relay(g):
        for half in range(2):
            relay_in(g, half).wait_recv()
            relay_out(g, half).start()

    last = ((2, 2), (1, 3), (3, 3), (2, 3))
    run_units(4, lambda u: (3 - u, 0), last, finish=finish)
    run_units(
        4, lambda u: (3 - u, 1), last, finish=finish,
        events=(
            (0, on_core(0, o3_far, 1, 2)),
            (1, lambda: relay(0)),
            (1, on_core(1, o3_pass_on, 2)),
            (2, on_core(1, o3_far, 3, 1)),
        ),
    )
    relay(1)
    on_core(1, o3_far, 2)()
    def out_terms(n, who):
        zc, yc = n // 2, (n % 2) * 2
        total = None
        for r in who:
            zs = ring(z, r)
            for i in range(2):
                src = AO.at[0] if r == 0 else ATT.at[zs]
                lhs = jnp.concatenate([src[2 * i], src[2 * i + 1]], axis=1)
                if i == 0:
                    cols = [WO[0, zs, yc, zc], WO[0, zs, yc + 1, zc]]
                else:
                    cols = [WO[1, zs, zc, yc], WO[1, zs, zc, yc + 1]]
                d = jnp.dot(lhs, jnp.concatenate(cols, axis=1), preferred_element_type=F32)
                total = d if total is None else total + d
        return total

    def own_block(zc, carry):
        for half in range(2):
            OF[2 * zc + half] = out_terms(2 * zc + half, (0,))
        return carry

    def out_copy(zc):
        cols = pl.ds(pl.multiple_of(zc * 512, 512), 512)
        return pltpu.make_async_copy(OB.at[zc], out_ref.at[:, cols], out_s.at[zc])

    def out_block(zc, carry):
        for half in range(2):
            total = OF[2 * zc + half] + out_terms(2 * zc + half, (1, 3, 2))
            OB[zc, :, half * 256:(half + 1) * 256] = total.astype(BF)
        out_copy(zc).start()
        return carry

    for r in range(4):
        for d in range(4):
            op_in(r, d).wait_recv()
    lax.fori_loop(0, 4, own_block, 0)
    for v in range(1, 4):
        for g in range(2):
            for half in range(2):
                at_in(v, g, half).wait_recv()
    lax.fori_loop(0, 4, out_block, 0)
    for i in range(6):
        tok(i).wait_send()
    for d in (1, 2, 3):
        o1(d).wait_send()
    w1[1].out(0).wait_send()
    w1[1].out(1).wait_send()
    w1_across().wait_send()
    for k in range(4):
        for stage in (w1[0], o2, *o3, *w2[0], *w2[1]):
            stage.out(k).wait_send()
        for r in range(4):
            op(r, k).wait_send()
            wp(0, r, k).wait_send()
            wp(1, r, k).wait_send()
    for v in range(4):
        for i in range(6):
            kvc(v, i).wait_send()
    for v in range(1, 4):
        for g in range(2):
            for half in range(2):
                (relay_out if v == 3 else functools.partial(at, v))(g, half).wait_send()
    for g in range(2):
        for half in range(2):
            relay_in(g, half).wait_send()
    for n in range(4):
        out_copy(n).wait()


def on_device(tokens, w_query, w_key, w_value, w_out, qk_gain):
    cos_t, sin_t = rope_tables()
    any_ = pl.BlockSpec(memory_space=pl.ANY)
    vm = pl.BlockSpec(memory_space=pltpu.VMEM)
    dma = pltpu.SemaphoreType.DMA
    pair = lambda *shape: [dma(shape), dma(shape)]
    out = pl.pallas_call(
        kernel,
        out_shape=jax.ShapeDtypeStruct((ROWS, 2048), BF),
        in_specs=[any_] * 8,
        out_specs=any_,
        scratch_shapes=[
            pltpu.VMEM((2, HD), F32),
            pltpu.VMEM((GRID_W, HD), F32),
            pltpu.VMEM((GRID_W, HD), F32),
            pltpu.VMEM((4, ROWS, 2048), BF),
            pltpu.VMEM((8, 4, 2, ROWS, HD), BF),
            pltpu.VMEM((2, 4, 4, 4, ROWS, HD), BF),
            pltpu.VMEM((4, 4, HD, ROWS), BF),
            pltpu.VMEM((16, 2, 2, ROWS, HD), BF),
            pltpu.VMEM((2, 8, ROWS, ROWS), F32),
            pltpu.VMEM((16, HD, ROWS), F32),
            pltpu.VMEM((16, 8, ROWS), F32),
            pltpu.VMEM((16, 8, ROWS), F32),
            pltpu.VMEM((4, 4, ROWS, HD), BF),
            pltpu.VMEM((4, 4, ROWS, HD), BF),
            pltpu.VMEM((2, 4, 128, HD), BF),
            pltpu.VMEM((8, ROWS, 256), F32),
            pltpu.VMEM((4, ROWS, 512), BF),
            dma((10,)),
            *pair(6), *pair(2, 4), *pair(2, 4, 4), *pair(2, 4, 4),
            *pair(3), *pair(4), *pair(4, 4), *pair(4, 4),
            *pair(4, 6), *pair(3, 2, 2), *pair(2, 2), dma((4,)),
        ],
        compiler_params=pltpu.CompilerParams(
            collective_id=0, has_side_effects=True, vmem_limit_bytes=56 * 1024 * 1024
        ),
    )(tokens, w_query, w_key.T, w_value.T, w_out, qk_gain, jnp.asarray(cos_t), jnp.asarray(sin_t))
    return out[None]


def solution(mesh):
    in_specs = (
        P("dp", "sp", None),
        P("dp", "sp"),
        P("dp", "sp"),
        P("dp", "sp"),
        P("dp", "sp"),
        P(),
    )
    out_specs = P("dp", "sp", None)
    return jax.shard_map(
        on_device, mesh=mesh, in_specs=in_specs, out_specs=out_specs, check_vma=False
    )
```

```python
import functools
import math

import jax
import jax.numpy as jnp
import numpy as np
from jax import lax
from jax.experimental import pallas as pl
from jax.experimental.pallas import tpu as pltpu
from jax.sharding import PartitionSpec as P

HQ = 16
KV = 8
HD = 128
GRID_W = 64
ROPE_BASE = 10000.0
EPS = 1e-06
ROWS = 256
BF = jnp.bfloat16
F32 = jnp.float32


def rope_tables():
    quarter = np.arange(0, HD // 2, 2, dtype=np.float32)
    inv_freq = np.float32(ROPE_BASE) ** (-quarter / np.float32(HD // 2))
    angle = np.arange(GRID_W, dtype=np.float32)[:, None] * inv_freq.astype(np.float32)
    angle = np.repeat(angle, 2, axis=1).astype(np.float64)
    angle = np.concatenate([angle, angle], axis=1)
    return np.cos(angle).astype(np.float32), np.sin(angle).astype(np.float32)


class Ring:
    def __init__(self, copy, slot, half, step, send, recv):
        self.copy, self.slot, self.half, self.step = copy, slot, half, step
        self.send, self.recv = send, recv

    def out(self, k):
        if k == 0 or k == 1:
            block = self.slot(0)
        elif k == 2:
            block = self.half(self.slot(3), 0)
        else:
            block = self.half(self.slot(1), 1)
        return self.copy(block, block, self.send(k), self.recv(k), **self.step(1 if k % 2 == 0 else 3))

    def into(self, k):
        far = self.slot(2)
        block = (self.slot(3), self.slot(1), self.half(far, 0), self.half(far, 1))[k]
        return self.copy(block, block, self.send(k), self.recv(k), **self.step(1))


def kernel(
    tok_hbm, wq_hbm, wk_hbm, wv_hbm, wo_hbm, gain_hbm, cos_hbm, sin_hbm,
    out_ref,
    gain_ref, cos_ref, sin_ref,
    X, W, WO, QT, KVB, S, ACC, MX, LS, AO, ATT, RB, OF, OB,
    loc, tok_s, tok_r, w1_s, w1_r, w2_s, w2_r, wp_s, wp_r,
    o1_s, o1_r, o2_s, o2_r, o3_s, o3_r, op_s, op_r,
    kv_s, kv_r, at_s, at_r, rl_s, rl_r, out_s,
):
    sp = lax.axis_index("sp")
    dp = lax.axis_index("dp")
    z, y = sp // 4, sp % 4
    x, c = dp // 2, dp % 2

    def ring(v, d):
        return (v + d + 4) % 4

    def device(dz=0, dy=0, dx=0, other=False):
        return {
            "sp": ring(z, dz) * 4 + ring(y, dy),
            "dp": ring(x, dx) * 2 + ((1 - c) if other else c),
        }

    def to(src, dst, ss, rs, **where):
        return pltpu.make_async_remote_copy(
            src_ref=src, dst_ref=dst, send_sem=ss, recv_sem=rs,
            device_id=device(**where), device_id_type=pl.DeviceIdType.MESH,
        )

    lo, hi = pl.ds(0, 128), pl.ds(128, 128)

    local = [
        (wq_hbm, W.at[dp, y, 0]),
        (wk_hbm.at[:, lo], W.at[dp, y, 1, pl.ds(0, 64)]),
        (wk_hbm.at[:, hi], W.at[dp, y, 1, pl.ds(128, 64)]),
        (wv_hbm.at[:, lo], W.at[dp, y, 1, pl.ds(64, 64)]),
        (wv_hbm.at[:, hi], W.at[dp, y, 1, pl.ds(192, 64)]),
        (wo_hbm, WO.at[c, x, y * (1 - c) + z * c, z * (1 - c) + y * c]),
        (tok_hbm.at[0], X.at[0]),
        (gain_hbm, gain_ref),
        (cos_hbm, cos_ref),
        (sin_hbm, sin_ref),
    ]
    local = [pltpu.make_async_copy(a, b, loc.at[i]) for i, (a, b) in enumerate(local)]
    for one in local:
        one.start()

    barrier = pltpu.get_barrier_semaphore()
    for where in (
        dict(dz=1), dict(dz=3), dict(dz=2), dict(dy=1), dict(dy=3), dict(dy=2), dict(dx=1),
        dict(dx=3), dict(dx=2), dict(other=True),
    ):
        pl.semaphore_signal(
            barrier, inc=1, device_id=device(**where), device_id_type=pl.DeviceIdType.MESH
        )
    pl.semaphore_wait(barrier, 10)

    def tok(i):
        dst = (X.at[1, lo], X.at[1, hi], X.at[2, hi], X.at[2, lo], X.at[3, lo], X.at[3, hi])[i]
        src = (
            tok_hbm.at[0, lo], tok_hbm.at[0, hi], tok_hbm.at[0, hi], tok_hbm.at[0, lo],
            X.at[1, lo], X.at[1, hi],
        )[i]
        return to(src, dst, tok_s.at[i], tok_r.at[i], dz=1 if i % 2 == 0 else 3)

    def set_off(v, half):
        gray = v ^ (v >> 1)
        return gray if half else (4 - gray) % 4

    def wslot(cc, d1, d2, part):
        cc1 = cc * part
        return W.at[
            ring(x, d2 * (1 - cc1) + d1 * cc1) * 2 + cc, ring(y, d1 * (1 - cc1) + d2 * cc1), part
        ]

    first_half = lambda ref, i: ref.at[i]
    row_half = lambda ref, i: ref.at[hi if i else lo]
    w1 = [
        Ring(
            to, lambda d, p=p: wslot(c, d, 0, p), row_half,
            lambda d, p=p: dict(dy=d * (1 - c * p), dx=d * c * p),
            lambda k, p=p: w1_s.at[p, k], lambda k, p=p: w1_r.at[p, k],
        )
        for p in range(2)
    ]
    w2 = [
        [
            Ring(
                to, lambda d, r=r, p=p: wslot(c, r, d, p), row_half,
                lambda d, p=p: dict(dy=d * c * p, dx=d * (1 - c * p)),
                lambda k, r=r, p=p: w2_s.at[p, r, k], lambda k, r=r, p=p: w2_r.at[p, r, k],
            )
            for r in range(4)
        ]
        for p in range(2)
    ]

    def wp(p, r, d):
        b = wslot(c, r, d, p)
        return to(b, b, wp_s.at[p, r, d], wp_r.at[p, r, d], other=True)

    def wp_in(p, r, d):
        b = wslot(1 - c, r, d, p)
        return to(b, b, wp_s.at[p, r, d], wp_r.at[p, r, d], other=True)

    oa, ob, oc = x, y * (1 - c) + z * c, z * (1 - c) + y * c

    def o1(d):
        return to(
            wo_hbm, WO.at[c, oa, ob, oc], o1_s.at[d - 1], o1_r.at[d - 1],
            dz=d * (1 - c), dy=d * c,
        )

    def o1_in(d):
        b = WO.at[c, oa, ob, ring(oc, -d)]
        return to(b, b, o1_s.at[d - 1], o1_r.at[d - 1], dz=1)

    two = lambda ref, i: ref.at[pl.ds(2 * i, 2)]
    o2 = Ring(
        to, lambda d: WO.at[c, oa, ring(ob, d)], two,
        lambda d: dict(dy=d * (1 - c), dz=d * c), lambda k: o2_s.at[k], lambda k: o2_r.at[k],
    )
    o3 = [
        Ring(
            to, lambda d, r=r: WO.at[c, ring(oa, d), ring(ob, r)], two,
            lambda d: dict(dx=d), lambda k, r=r: o3_s.at[r, k], lambda k, r=r: o3_r.at[r, k],
        )
        for r in range(4)
    ]

    def op(r, d):
        b = WO.at[c, ring(oa, d), ring(ob, r)]
        return to(b, b, op_s.at[r, d], op_r.at[r, d], other=True)

    def op_in(r, d):
        b = WO.at[1 - c, ring(oa, d), ring(y * c + z * (1 - c), r)]
        return to(b, b, op_s.at[r, d], op_r.at[r, d], other=True)

    def kvc(v, i, landing=False):
        half = (0, 1, 1, 0, 0, 1)[i]
        from_y = ((3, 3, 1, 1, 2, 2) if landing else (0, 0, 0, 0, 3, 1))[i]
        b = KVB.at[ring(y, from_y) * 4 + v, half]
        return to(b, b, kv_s.at[v, i], kv_r.at[v, i], dy=(1, 1, 3, 3, 1, 3)[i])

    def at(v, g, half):
        rows, heads = hi if half else lo, pl.ds(2 * g, 2)
        return to(
            AO.at[v, heads, rows], ATT.at[z, heads, rows],
            at_s.at[v - 1, g, half], at_r.at[v - 1, g, half], dz=set_off(v, half),
        )

    def at_in(v, g, half):
        b = ATT.at[ring(z, -set_off(v, half)), pl.ds(2 * g, 2), hi if half else lo]
        return to(b, b, at_s.at[v - 1, g, half], at_r.at[v - 1, g, half], dz=1)

    def relay_in(g, half):
        heads = pl.ds(2 * g, 2)
        return to(
            AO.at[3, heads, hi if half else lo], RB.at[half, heads],
            rl_s.at[g, half], rl_r.at[g, half], dz=3 if half else 1,
        )

    def relay_out(g, half):
        heads = pl.ds(2 * g, 2)
        return to(
            RB.at[half, heads], ATT.at[ring(z, 1 if half else 3), heads, hi if half else lo],
            at_s.at[2, g, half], at_r.at[2, g, half], dz=3 if half else 1,
        )

    def w1_near(p):
        for k in range(2):
            w1[p].into(k).wait_recv()
            if p == 0:
                w1[p].out(k + 2).start()

    def w1_far(p):
        if p == 0:
            w1[p].into(2).wait_recv()
            w1[p].into(3).wait_recv()
        else:
            w1_across(True).wait_recv()

    def w1_across(landing=False):
        b = wslot(c, 2 if landing else 0, 0, 1)
        return to(b, b, w1_s.at[1, 2], w1_r.at[1, 2], dy=2 * (1 - c), dx=2 * c)

    def w2_send(p, r):
        w2[p][r].out(0).start()
        w2[p][r].out(1).start()
        wp(p, r, 0).start()

    def w2_near(p, r):
        for k in range(2):
            w2[p][r].into(k).wait_recv()
            w2[p][r].out(k + 2).start()
            wp(p, r, 3 if k == 0 else 1).start()

    def w2_far(p, r):
        w2[p][r].into(2).wait_recv()
        w2[p][r].into(3).wait_recv()
        wp(p, r, 2).start()

    def wp_wait(p):
        for r in (0, 3, 1, 2):
            for d in (0, 3, 1, 2):
                wp_in(p, r, d).wait_recv()

    def o1_send():
        for d in (2, 1, 3):
            o1(d).start()

    pl.when(c == 0)(o1_send)
    for i in range(4):
        tok(i).start()
    for i in range(4):
        local[i + 1].wait()
    w1[1].out(0).start()
    w1[1].out(1).start()
    w1_across().start()
    local[0].wait()
    w1[0].out(0).start()
    w1[0].out(1).start()
    ACC[...] = jnp.zeros_like(ACC)
    LS[...] = jnp.zeros_like(LS)
    MX[...] = jnp.full(MX.shape, -jnp.inf, F32)
    def o3_send(r):
        o3[r].out(0).start()
        o3[r].out(1).start()
        op(r, 0).start()

    def o2_send():
        local[5].wait()
        for d in (1, 3, 2):
            o1_in(d).wait_recv()
        o2.out(0).start()
        o2.out(1).start()

    def o2_pass_on():
        for k in range(2):
            o2.into(k).wait_recv()
            o2.out(k + 2).start()
            o3_send(3 if k == 0 else 1)

    order = (0, 3, 1, 2)
    w1_near(1)
    for r in order[:3]:
        w2_send(1, r)
    w1_far(1)
    w2_send(1, 2)
    w1_near(0)
    pl.when(c == 0)(o2_send)
    for r in order:
        w2_near(1, r)
    w1_far(0)
    for r in order:
        w2_send(0, r)
    pl.when(c == 1)(o1_send)
    for r in order:
        w2_far(1, r)
    wp_wait(1)
    for i in range(6, 10):
        local[i].wait()
    lane = lax.broadcasted_iota(jnp.int32, (64, HD), 1)
    low64 = lane < 64
    even = lane % 2 == 0

    def normed_turned(raw, gain, cosv, sin_a, sin_b):
        n = raw * lax.rsqrt(jnp.mean(raw * raw, axis=1, keepdims=True) + EPS) * gain
        return n * cosv + (pltpu.roll(n, HD - 1, 1) * sin_a + pltpu.roll(n, 1, 1) * sin_b)

    def turns_of(v):
        turns = []
        for g in range(4):
            row = (ring(z, set_off(v, g // 2)) * 4 + y) * 4 + g
            cosv = jnp.where(low64, cos_ref[pl.ds(row, 1), :], cos_ref[...])
            sinv = jnp.where(low64, sin_ref[pl.ds(row, 1), :], sin_ref[...])
            turns.append((cosv, jnp.where(even, -sinv, 0.0), jnp.where(even, 0.0, sinv)))
        return turns

    def project_q(v):
        gq = gain_ref[0:1, :]
        turns = turns_of(v)
        for j in range(2):
            raw = jnp.zeros((ROWS, ROWS), F32)
            for k in range(8):
                rq = jnp.concatenate([W[k, 2 * j, 0], W[k, 2 * j + 1, 0]], axis=1)
                raw = raw + jnp.dot(
                    X[v, :, k * 256:(k + 1) * 256], rq, preferred_element_type=F32
                )
            for g in range(4):
                sl = slice(g * 64, (g + 1) * 64)
                for b in range(2):
                    S[j, b, sl, 0:HD] = normed_turned(
                        raw[sl, b * HD:(b + 1) * HD], gq, *turns[g]
                    )
            for half in range(2):
                hs = slice(half * 128, (half + 1) * 128)
                for b in range(2):
                    QT[v, 2 * j + b, :, hs] = S[j, b, hs, 0:HD].T.astype(BF)

    def project_kv(v):
        chunk = y * 4 + v
        gk = gain_ref[1:2, :]
        turns = turns_of(v)
        for j in range(2):
            raw = jnp.zeros((ROWS, ROWS), F32)
            for k in range(8):
                rkv = jnp.concatenate(
                    [
                        jnp.concatenate([W[k, b, 1, 0:128], W[k, b, 1, 128:256]], axis=1)
                        for b in (2 * j, 2 * j + 1)
                    ],
                    axis=0,
                )
                raw = raw + lax.dot_general(
                    X[v, :, k * 256:(k + 1) * 256], rkv, (((1,), (1,)), ((), ())),
                    preferred_element_type=F32,
                )
            for g in range(4):
                sl = slice(g * 64, (g + 1) * 64)
                a0 = raw[sl, 0:HD]
                a1 = raw[sl, HD:]
                kk = jnp.where(low64, a0, pltpu.roll(a1, 64, 1))
                KVB[chunk, j, 0, sl, :] = normed_turned(kk, gk, *turns[g]).astype(BF)
                S[j, 2, sl, 0:HD] = jnp.where(low64, pltpu.roll(a0, 64, 1), a1)
            for half in range(2):
                hs = slice(half * 128, (half + 1) * 128)
                KVB[chunk, j, 1, hs, :] = S[j, 2, hs, 0:HD].T.astype(BF)

    def kv_and_send(v):
        project_kv(v)
        for i in (0, 2, 1, 3):
            kvc(v, i).start()

    def kv_pass_on(v):
        for i in (0, 2):
            kvc(v, i, True).wait_recv()
            kvc(v, 4 + i // 2).start()

    def kv_near(v):
        for i in (1, 3):
            kvc(v, i, True).wait_recv()

    def kv_far(v):
        for i in (4, 5):
            kvc(v, i, True).wait_recv()

    cs = HD ** (-0.5) * math.log2(math.e)
    NEG = jnp.full((8, 256), -jnp.inf, F32)

    def run_units(n, unit_of, chunks, finish=None, events=()):
        refs = [ring(y, dy) * 4 + v for dy, v in chunks]

        def scores(u, j, b, m8):
            v, g = unit_of(u)
            s = jnp.dot(KVB[refs[j], g, 0], QT[v, 2 * g + b], preferred_element_type=F32)
            S[b, j] = s
            return jnp.maximum(m8, jnp.max(s.reshape(32, 8, 256), axis=0))

        def unit(u, m8s, more):
            v, g = unit_of(u)
            news = [NEG, NEG]
            for b in range(2):
                t = v * 4 + 2 * g + b
                m_old = MX[t]
                m = jnp.maximum(
                    m_old, jnp.broadcast_to(jnp.max(m8s[b], axis=0, keepdims=True), (8, 256))
                )
                alpha = jnp.exp2((m_old - m) * cs)
                l8 = LS[t] * alpha
                pv = None
                for j in range(len(refs)):
                    p = jnp.exp2((S[b, j].reshape(32, 8, 256) - m[None]) * cs)
                    l8 = l8 + jnp.sum(p, axis=0)
                    vt = jnp.concatenate(
                        [KVB[refs[j], g, 1, 0:128, :], KVB[refs[j], g, 1, 128:256, :]], axis=1
                    )
                    d = jnp.dot(vt, p.reshape(256, 256).astype(BF), preferred_element_type=F32)
                    pv = d if pv is None else pv + d
                    if more:
                        news[b] = scores(u + 1, j, b, news[b])
                acc = (ACC[t].reshape(16, 8, 256) * alpha[None]).reshape(HD, ROWS) + pv
                if finish is None:
                    MX[t] = m
                    LS[t] = l8
                    ACC[t] = acc
                else:
                    o = acc * (1.0 / jnp.sum(l8, axis=0, keepdims=True))
                    AO[v, 2 * g + b] = o.astype(BF).T
            if finish is not None:
                finish(v, g)
            return tuple(news)

        m8s = [NEG, NEG]
        for j in range(len(refs)):
            for b in range(2):
                m8s[b] = scores(0, j, b, m8s[b])

        def step(u, m8s):
            m8s = unit(u, m8s, True)
            for when, event in events:
                pl.when(u == when)(event)
            return m8s

        unit(n - 1, lax.fori_loop(0, n - 1, step, tuple(m8s)), False)

    def finish(v, g):
        @pl.when(v != 3)
        def _():
            @pl.when(v != 0)
            def _():
                at(v, g, 0).start()
                at(v, g, 1).start()

        @pl.when(v == 3)
        def _():
            relay_in(g, 0).start()
            relay_in(g, 1).start()

    def o2_far():
        o2.into(2).wait_recv()
        o2.into(3).wait_recv()
        o3_send(2)

    def o3_pass_on(*rs):
        for r in rs:
            for k in range(2):
                o3[r].into(k).wait_recv()
                o3[r].out(k + 2).start()
                op(r, 3 if k == 0 else 1).start()

    def o3_far(*rs):
        for r in rs:
            o3[r].into(2).wait_recv()
            o3[r].into(3).wait_recv()
            op(r, 2).start()

    def q_step(v, carry):
        project_q(v)
        return carry

    kv_and_send(0)
    for r in order:
        w2_near(0, r)
    pl.when(c == 0)(lambda: o3_send(0))
    for i in range(2):
        tok(i).wait_recv()
        tok(i + 4).start()

    @pl.when(c == 1)
    def _():
        o2_send()
        o3_send(0)
    kv_and_send(1)
    pl.when(c == 0)(o2_pass_on)
    for r in order:
        w2_far(0, r)
    wp_wait(0)
    lax.fori_loop(0, 2, q_step, 0)
    first_two = lambda u: (u // 2, u % 2)
    set_a = ((0, 0), (0, 1))
    set_b = ((0, 2), (1, 0), (3, 0))
    set_d = ((2, 0), (1, 1), (3, 1))
    run_units(4, first_two, set_a)
    kv_pass_on(0)
    kv_near(0)
    tok(2).wait_recv()
    tok(3).wait_recv()
    kv_and_send(2)
    project_q(2)
    run_units(4, first_two, set_b)
    run_units(2, lambda u: (2, u), set_a + set_b)
    pl.when(c == 0)(o2_far)
    kv_pass_on(1)
    kv_near(1)
    kv_far(0)
    o3_pass_on(0)
    pl.when(c == 0)(lambda: o3_pass_on(3))
    run_units(6, first_two, set_d)
    tok(4).wait_recv()
    tok(5).wait_recv()
    kv_and_send(3)
    pl.when(c == 1)(o2_pass_on)
    project_q(3)

    def on_core(core, event, *rs):
        return lambda: pl.when(c == core)(lambda: event(*rs))

    run_units(2, lambda u: (3, u), set_a + set_b + set_d)
    kv_pass_on(2)
    kv_near(2)
    kv_far(1)

    run_units(
        8, first_two, ((0, 3), (2, 1), (1, 2), (3, 2)),
        events=(
            (0, on_core(0, o3_pass_on, 1, 2)),
            (0, on_core(1, o2_far)),
            (2, lambda: kv_pass_on(3)),
            (5, lambda: o3_far(0)),
            (5, on_core(0, o3_far, 3)),
        ),
    )
    kv_far(2)
    kv_near(3)
    kv_far(3)

    def relay(g):
        for half in range(2):
            relay_in(g, half).wait_recv()
            relay_out(g, half).start()

    last = ((2, 2), (1, 3), (3, 3), (2, 3))
    run_units(
        4, lambda u: (3 - u, 0), last, finish=finish,
        events=((0, on_core(1, o3_pass_on, 3, 1)),),
    )
    run_units(
        4, lambda u: (3 - u, 1), last, finish=finish,
        events=(
            (0, on_core(0, o3_far, 1, 2)),
            (1, lambda: relay(0)),
            (1, on_core(1, o3_pass_on, 2)),
            (2, on_core(1, o3_far, 3, 1)),
        ),
    )
    relay(1)
    on_core(1, o3_far, 2)()
    def out_terms(n, who):
        zc, yc = n // 2, (n % 2) * 2
        total = None
        for r in who:
            zs = ring(z, r)
            for i in range(2):
                src = AO.at[0] if r == 0 else ATT.at[zs]
                lhs = jnp.concatenate([src[2 * i], src[2 * i + 1]], axis=1)
                if i == 0:
                    cols = [WO[0, zs, yc, zc], WO[0, zs, yc + 1, zc]]
                else:
                    cols = [WO[1, zs, zc, yc], WO[1, zs, zc, yc + 1]]
                d = jnp.dot(lhs, jnp.concatenate(cols, axis=1), preferred_element_type=F32)
                total = d if total is None else total + d
        return total

    def own_block(zc, carry):
        for half in range(2):
            OF[2 * zc + half] = out_terms(2 * zc + half, (0,))
        return carry

    def out_copy(zc):
        cols = pl.ds(pl.multiple_of(zc * 512, 512), 512)
        return pltpu.make_async_copy(OB.at[zc], out_ref.at[:, cols], out_s.at[zc])

    def out_block(zc, carry):
        for half in range(2):
            total = OF[2 * zc + half] + out_terms(2 * zc + half, (1, 3, 2))
            OB[zc, :, half * 256:(half + 1) * 256] = total.astype(BF)
        out_copy(zc).start()
        return carry

    for r in range(4):
        for d in range(4):
            op_in(r, d).wait_recv()
    lax.fori_loop(0, 4, own_block, 0)
    for v in range(1, 4):
        for g in range(2):
            for half in range(2):
                at_in(v, g, half).wait_recv()
    lax.fori_loop(0, 4, out_block, 0)
    for i in range(6):
        tok(i).wait_send()
    for d in (1, 2, 3):
        o1(d).wait_send()
    w1[1].out(0).wait_send()
    w1[1].out(1).wait_send()
    w1_across().wait_send()
    for k in range(4):
        for stage in (w1[0], o2, *o3, *w2[0], *w2[1]):
            stage.out(k).wait_send()
        for r in range(4):
            op(r, k).wait_send()
            wp(0, r, k).wait_send()
            wp(1, r, k).wait_send()
    for v in range(4):
        for i in range(6):
            kvc(v, i).wait_send()
    for v in range(1, 4):
        for g in range(2):
            for half in range(2):
                (relay_out if v == 3 else functools.partial(at, v))(g, half).wait_send()
    for g in range(2):
        for half in range(2):
            relay_in(g, half).wait_send()
    for n in range(4):
        out_copy(n).wait()


def on_device(tokens, w_query, w_key, w_value, w_out, qk_gain):
    cos_t, sin_t = rope_tables()
    any_ = pl.BlockSpec(memory_space=pl.ANY)
    vm = pl.BlockSpec(memory_space=pltpu.VMEM)
    dma = pltpu.SemaphoreType.DMA
    pair = lambda *shape: [dma(shape), dma(shape)]
    out = pl.pallas_call(
        kernel,
        out_shape=jax.ShapeDtypeStruct((ROWS, 2048), BF),
        in_specs=[any_] * 8,
        out_specs=any_,
        scratch_shapes=[
            pltpu.VMEM((2, HD), F32),
            pltpu.VMEM((GRID_W, HD), F32),
            pltpu.VMEM((GRID_W, HD), F32),
            pltpu.VMEM((4, ROWS, 2048), BF),
            pltpu.VMEM((8, 4, 2, ROWS, HD), BF),
            pltpu.VMEM((2, 4, 4, 4, ROWS, HD), BF),
            pltpu.VMEM((4, 4, HD, ROWS), BF),
            pltpu.VMEM((16, 2, 2, ROWS, HD), BF),
            pltpu.VMEM((2, 8, ROWS, ROWS), F32),
            pltpu.VMEM((16, HD, ROWS), F32),
            pltpu.VMEM((16, 8, ROWS), F32),
            pltpu.VMEM((16, 8, ROWS), F32),
            pltpu.VMEM((4, 4, ROWS, HD), BF),
            pltpu.VMEM((4, 4, ROWS, HD), BF),
            pltpu.VMEM((2, 4, 128, HD), BF),
            pltpu.VMEM((8, ROWS, 256), F32),
            pltpu.VMEM((4, ROWS, 512), BF),
            dma((10,)),
            *pair(6), *pair(2, 4), *pair(2, 4, 4), *pair(2, 4, 4),
            *pair(3), *pair(4), *pair(4, 4), *pair(4, 4),
            *pair(4, 6), *pair(3, 2, 2), *pair(2, 2), dma((4,)),
        ],
        compiler_params=pltpu.CompilerParams(
            collective_id=0, has_side_effects=True, vmem_limit_bytes=56 * 1024 * 1024
        ),
    )(tokens, w_query, w_key.T, w_value.T, w_out, qk_gain, jnp.asarray(cos_t), jnp.asarray(sin_t))
    return out[None]


def solution(mesh):
    in_specs = (
        P("dp", "sp", None),
        P("dp", "sp"),
        P("dp", "sp"),
        P("dp", "sp"),
        P("dp", "sp"),
        P(),
    )
    out_specs = P("dp", "sp", None)
    return jax.shard_map(
        on_device, mesh=mesh, in_specs=in_specs, out_specs=out_specs, check_vma=False
    )
```
